512 devices in a mesh: kv: 64 (over z, y), tp: 8 (over x, core).
Axes of the slice: x: 4, y: 8, z: 8, core: 2. Of those that a mesh axis runs over, the one named last changes fastest.
Arguments:
- queries: bfloat16 [8192, 1024], P('kv', 'tp'), may hold values from -4 to 4
- keys: bfloat16 [8192, 1024], P('kv', 'tp'), may hold values from -4 to 4
- values: bfloat16 [8192, 1024], P('kv', 'tp'), may hold values from -4 to 4
- cotangent: bfloat16 [8192, 1024], P('kv', 'tp'), may hold values from -4 to 4
- log_sum: float32 [16, 8192], P('tp', 'kv'), may hold values from 4.5 to 7.5
- chosen: int32 [16, 256, 12], P('tp'), may hold values from 0 to 255, as said below
- normed_input: bfloat16 [8192, 2048], P('kv', 'tp'), may hold values from -0.0625 to 0.0625
Outputs:
- grad_queries: bfloat16 [8192, 1024], P('kv', 'tp')
- grad_keys: bfloat16 [8192, 1024], P('kv', 'tp')
- grad_values: bfloat16 [8192, 1024], P('kv', 'tp')
- grad_weight: float32 [2048, 1024], P('kv', 'tp')
The draws below stay inside these ranges and needn't reach their ends.
Inputs may be any that keep to these rules, and one draw needn't show every extreme that they name: `chosen`: for each head, the distinct blocks below their own query block that the query blocks of one device's 128 positions choose include at most 1 block of any one device's span of 128 positions, and exactly 1 for some pairs of devices. Within one list the entries below the query block's own index are distinct.
All inputs are finite; a program needn't handle non-finite values.
Results may differ from the reference program's by a relative error of at most 0.0085.
Values may be sent and summed in bfloat16 or wider, within the bound.
A program may use at most 64 MiB of HBM per device.

```python
import jax
import jax.numpy as jnp
from jax import lax

D = 2048
HEADS = 16
HD = 64
BLK = 32
SEL = 12
MOST = 1
TOK_DEV = 128
TOKENS = 8192
WIDTH = 1024
N_KV = 64


def draw_chosen(key, part):
    devices = N_KV
    blocks_dev = TOK_DEV // BLK
    splits = jax.random.split(jax.random.fold_in(key, 17), 4)
    first_pick = jax.random.randint(splits[0], (HEADS, devices, devices), 0, blocks_dev)
    step_pick = jax.random.randint(splits[1], (HEADS, devices, devices), 1, blocks_dev)
    owner_ids = jnp.arange(devices, dtype=jnp.int32)
    cand_list = []
    for slot_index in range(MOST):
        local_pick = (first_pick + slot_index * step_pick) % blocks_dev
        cand_list.append(owner_ids[None, None, :] * blocks_dev + local_pick)
    candidates = jnp.stack(cand_list, axis=-1)
    popular = jax.random.randint(splits[2], (HEADS, 1, devices, 1), 0, 8)
    popular = popular * popular
    query_dev = owner_ids[None, :, None, None]
    owner_dev = owner_ids[None, None, :, None]
    boosted = jnp.where((owner_dev == query_dev - 1) | (owner_dev == query_dev - devices // 2), 2, 0)
    base_score = boosted * 64 + popular
    jitter = jax.random.randint(splits[3], (HEADS, devices, blocks_dev, devices, MOST), 0, 4096)
    query_ids = owner_ids[:, None] * blocks_dev + jnp.arange(blocks_dev, dtype=jnp.int32)[None, :]
    cand_rows = candidates[:, :, None, :, :]
    usable = cand_rows < query_ids[None, :, :, None, None]
    tie_break = jnp.arange(MOST * devices, dtype=jnp.int32).reshape(devices, MOST)
    scored = (base_score[:, :, None, :, :] * 4096 + jitter) * 256 + tie_break
    scored = jnp.where(usable, scored, -1).reshape(HEADS, devices, blocks_dev, MOST * devices)
    top_values, top_index = lax.top_k(scored, SEL)
    flat_cands = jnp.broadcast_to(cand_rows, (HEADS, devices, blocks_dev, devices, MOST)).reshape(HEADS, devices, blocks_dev, MOST * devices)
    picked = jnp.take_along_axis(flat_cands, top_index, axis=-1)
    picked = jnp.where(top_values >= 0, picked, query_ids[None, :, :, None])
    return picked.reshape(HEADS, devices * blocks_dev, SEL).astype(jnp.int32)


def block_levels(stream_key, shape, cuts, low, largest):
    level, own = 1.0, jax.random.fold_in(stream_key, 6)
    for dim, blocks in cuts:
        draws = jnp.exp(jax.random.uniform(jax.random.fold_in(own, dim), (blocks,), jnp.float32, low / len(cuts), largest / len(cuts)))
        level = level * jnp.repeat(draws, shape[dim] // blocks).reshape([-1 if axis == dim else 1 for axis in range(len(shape))])
    return level


def noise(own_key, shape, scale, most, pieces=(), kind=jnp.bfloat16):
    gain = block_levels(own_key, shape, pieces, -0.22, 0.18) if pieces else 1.0
    array = jax.random.normal(own_key, shape, jnp.float32) * scale * gain
    return jnp.minimum(jnp.maximum(array, -most), most).astype(kind)


def setup_inputs(seed: int = 0) -> dict:
    key_list = jax.random.split(jax.random.key(seed), 8)
    queries = noise(key_list[0], (TOKENS, WIDTH), 1.0, 4.0, ((0, 64), (1, 8)))
    keys = noise(key_list[1], (TOKENS, WIDTH), 1.0, 4.0, ((0, 64), (1, 8)))
    values = noise(key_list[2], (TOKENS, WIDTH), 1.0, 4.0, ((0, 64), (1, 8)))
    cotangent = noise(key_list[3], (TOKENS, WIDTH), 1.0, 4.0, ((0, 64), (1, 8)))
    log_sum = jnp.clip(4.5 + 3.0 * jax.random.uniform(key_list[4], (HEADS, TOKENS), jnp.float32) ** block_levels(key_list[4], (HEADS, TOKENS), ((0, 8), (1, 64)), -0.2, 0.2), 4.5, 7.5)
    chosen = draw_chosen(jax.random.fold_in(key_list[7], 71), 0)
    normed_input = noise(key_list[6], (TOKENS, D), TOKENS ** -0.5, 0.0625, ((0, 64), (1, 8)))
    return dict(queries=queries, keys=keys, values=values, cotangent=cotangent, log_sum=log_sum, chosen=chosen, normed_input=normed_input)


MASKED = -1e30


def reference(queries, keys, values, cotangent, log_sum, chosen, normed_input):
    token_count = queries.shape[0]
    block_total = token_count // BLK
    score_scale = HD ** -0.5
    block_ids = jnp.arange(block_total, dtype=jnp.int32)
    causal = jnp.arange(BLK)[:, None] >= jnp.arange(BLK)[None, :]

    def per_head(head_index):
        def columns(row_block):
            picked_cols = lax.dynamic_slice_in_dim(row_block, head_index * HD, HD, 1)
            return picked_cols.reshape(block_total, BLK, HD).astype(jnp.float32)

        q_blocks = columns(queries)
        k_blocks = columns(keys)
        v_blocks = columns(values)
        g_blocks = columns(cotangent)
        log_rows = lax.dynamic_index_in_dim(log_sum, head_index, 0, keepdims=False).reshape(block_total, BLK)[..., None]
        picked = lax.dynamic_index_in_dim(chosen, head_index, 0, keepdims=False).astype(jnp.int32)
        usable = picked < block_ids[:, None]
        safe_ids = jnp.where(usable, picked, 0).astype(jnp.int32)
        keys_all = jnp.concatenate([k_blocks[safe_ids].reshape(block_total, SEL * BLK, HD), k_blocks], axis=1)
        values_all = jnp.concatenate([v_blocks[safe_ids].reshape(block_total, SEL * BLK, HD), v_blocks], axis=1)
        sel_mask = jnp.broadcast_to(jnp.repeat(usable, BLK, axis=1)[:, None, :], (block_total, BLK, SEL * BLK))
        allowed = jnp.concatenate([sel_mask, jnp.broadcast_to(causal, (block_total, BLK, BLK))], axis=2)
        scores = jnp.einsum('jqd,jkd->jqk', q_blocks, keys_all) * score_scale
        weights = jnp.exp(jnp.where(allowed, scores - log_rows, MASKED))
        value_dots = jnp.einsum('jqd,jkd->jqk', g_blocks, values_all)
        row_delta = jnp.sum(weights * value_dots, axis=-1, keepdims=True)
        score_grad = lax.optimization_barrier((weights * (value_dots - row_delta)).astype(jnp.bfloat16)).astype(jnp.float32)
        weights_low = lax.optimization_barrier(weights.astype(jnp.bfloat16)).astype(jnp.float32)
        query_grad = jnp.einsum('jqk,jkd->jqd', score_grad, keys_all) * score_scale
        key_grad = jnp.einsum('jqk,jqd->jkd', score_grad, q_blocks) * score_scale
        value_grad = jnp.einsum('jqk,jqd->jkd', weights_low, g_blocks)

        def settle(gradient):
            spread = gradient[:, :SEL * BLK].reshape(block_total * SEL, BLK, HD)
            summed = jax.ops.segment_sum(spread, safe_ids.reshape(-1), num_segments=block_total)
            return (summed + gradient[:, SEL * BLK:]).reshape(token_count, HD).astype(jnp.bfloat16)

        return query_grad.reshape(token_count, HD).astype(jnp.bfloat16), settle(key_grad), settle(value_grad)

    head_grads = lax.map(per_head, jnp.arange(HEADS, dtype=jnp.int32))

    def joined_rows(stacked):
        return stacked.transpose(1, 0, 2).reshape(token_count, HEADS * HD)

    grad_queries = joined_rows(head_grads[0])
    grad_keys = joined_rows(head_grads[1])
    grad_values = joined_rows(head_grads[2])
    grad_weight = jnp.dot(normed_input.T, grad_queries, preferred_element_type=jnp.float32)
    return grad_queries, grad_keys, grad_values, grad_weight
```

```python
import jax
import jax.numpy as jnp
from jax import lax
from jax.experimental import pallas as pl
from jax.experimental.pallas import tpu as pltpu
from jax.sharding import PartitionSpec as P

HD = 64
BLK = 32
SEL = 12
MASKED = -1e30
RING = 8
TOK = 128
COLS = 128
OFFS = (0, 1, 7, 2, 6, 3, 5, 4)
MESH = pl.DeviceIdType.MESH
F32 = jnp.float32
BF16 = jnp.bfloat16


def nt(a, b):
    return lax.dot_general(a, b, (((1,), (1,)), ((), ())), preferred_element_type=F32)


def nn(a, b):
    return lax.dot_general(a, b, (((1,), (0,)), ((), ())), preferred_element_type=F32)


def kernel(
    q_in, k_in, v_in, g_in, ls_in, ch_in, x_in,
    dq_out, dk_out, dv_out, gw_out,
    qg, kv, ls, xg, chs, qm, gm, kt, xt, bias, wf, dpf, w16, ds16, dl,
    dvs, dvr, dks, dkr, dqs, dqr, gas, gar, gbs, gbr, ha_s, ha_r, hb_s, hb_r,
    loc, sq, rq, sl, rl, sk, rk, sx, rx, sd, rd, sv, rv, sdk, rdk, sdq, rdq,
    sga, rga, sgb, rgb, sha, rha, shb, rhb,
):
    me = lax.axis_index("kv")
    tp = lax.axis_index("tp")
    z = me // RING
    y = me % RING

    def ring(base, off):
        return (base + off) % RING

    def along_y(off):
        return (z * RING + ring(y, off), tp)

    def along_z(off):
        return (ring(z, off) * RING + y, tp)

    def along_tp(off):
        return (me, ring(tp, off))

    def remote(src, dst, send, recv, target):
        return pltpu.make_async_remote_copy(
            src_ref=src, dst_ref=dst, send_sem=send, recv_sem=recv, device_id=target, device_id_type=MESH
        )

    barrier = pltpu.get_barrier_semaphore()
    for off in range(1, RING):
        for target in (along_y(off), along_z(off), along_tp(off)):
            pl.semaphore_signal(barrier, inc=1, device_id=target, device_id_type=MESH)

    first, second = pl.ds(0, TOK), pl.ds(TOK, TOK)
    locals_ = [
        pltpu.make_async_copy(q_in, qg.at[y, first], loc.at[0]),
        pltpu.make_async_copy(g_in, qg.at[y, second], loc.at[1]),
        pltpu.make_async_copy(k_in, kv.at[z, first], loc.at[2]),
        pltpu.make_async_copy(v_in, kv.at[z, second], loc.at[3]),
        pltpu.make_async_copy(ls_in, ls.at[y], loc.at[4]),
        pltpu.make_async_copy(x_in, xg.at[tp], loc.at[5]),
        pltpu.make_async_copy(ch_in.at[:, pl.ds(z * 32, 32)], chs, loc.at[6]),
    ]
    for c in locals_:
        c.start()
    for c in locals_:
        c.wait()
    pl.semaphore_wait(barrier, 3 * (RING - 1))

    pending = []

    def send(src, dst, ssem, rsem, target):
        c = remote(src, dst, ssem, rsem, target)
        c.start()
        pending.append(c)

    for i, off in enumerate(OFFS[1:]):
        send(qg.at[y], qg.at[y], sq.at[i], rq.at[y], along_y(off))
        send(ls.at[y], ls.at[y], sl.at[i], rl.at[y], along_y(off))
        send(kv.at[z], kv.at[z], sk.at[i], rk.at[z], along_z(off))
    for i, off in enumerate(OFFS[1:]):
        send(xg.at[tp], xg.at[tp], sx.at[i], rx.at[tp], along_tp(off))

    spread = (
        lax.broadcasted_iota(jnp.int32, (32, 1024), 1) // BLK
        == lax.broadcasted_iota(jnp.int32, (32, 1024), 0)
    ).astype(BF16)
    own_id = (lax.broadcasted_iota(jnp.int32, (1, 1024), 1) // BLK + z * 32).astype(F32)
    for h in range(2):
        lists = lax.dot_general(
            chs[h].astype(F32).astype(BF16), spread, (((0,), (0,)), ((), ())), preferred_element_type=F32
        )

        def one_column(zz, _, h=h, lists=lists):
            block = ((zz * RING + y) * 4 + lax.broadcasted_iota(jnp.int32, (4, 1024), 0)).astype(F32)
            hit = jnp.zeros((4, 1024), F32)
            for s in range(SEL):
                hit = jnp.where(block == lists[s : s + 1, :], 1.0, hit)
            hit = jnp.where(block < own_id, hit, 0.0)
            hit = jnp.where(block == own_id, 1.0, hit)
            bias[h, zz] = jnp.where(hit > 0.5, 0.0, MASKED)
            return 0

        lax.fori_loop(0, RING, one_column, 0)

    head0 = lax.broadcasted_iota(jnp.int32, (TOK, COLS), 1) < HD
    zero = jnp.zeros((TOK, COLS), BF16)

    def stage_q(yy):
        for src, dst in ((first, qm), (second, gm)):
            tile = qg[yy, src, :]
            dst[yy, first, :] = jnp.where(head0, tile, zero)
            dst[yy, second, :] = jnp.where(head0, zero, tile)

    def stage_k(zz):
        tile = kv[zz, first, :]
        kt[:, pl.ds(pl.multiple_of(zz * TOK, TOK), TOK)] = tile.astype(F32).T.astype(BF16)

    for off in OFFS:
        if off:
            yy, zz = ring(y, off), ring(z, off)
            remote(qg.at[yy], qg.at[yy], sq.at[0], rq.at[yy], along_y(off)).wait_recv()
            remote(ls.at[yy], ls.at[yy], sl.at[0], rl.at[yy], along_y(off)).wait_recv()
            remote(kv.at[zz], kv.at[zz], sk.at[0], rk.at[zz], along_z(off)).wait_recv()

    def stage(i, _):
        stage_q(i)
        stage_k(i)
        return 0

    lax.fori_loop(0, RING, stage, 0)

    row_i = lax.broadcasted_iota(jnp.int32, (TOK, TOK), 0)
    col_i = lax.broadcasted_iota(jnp.int32, (TOK, TOK), 1)
    future = (row_i // BLK == col_i // BLK) & (row_i > col_i)
    diag_bias = jnp.where(future, MASKED, 0.0).astype(F32)
    dl[y] = jnp.zeros((16, TOK), F32)

    def strip(zz, _):
        k_tile = kv[zz, first, :]
        v_tile = kv[zz, second, :]
        for yy in range(RING):
            s = nt(k_tile, qm[yy])
            dp = nt(v_tile, gm[yy])
            own = jnp.where((zz == z) & (yy == y), 1.0, 0.0).astype(F32)
            for h in range(2):
                lanes = slice(h * TOK, (h + 1) * TOK)
                rows = bias[h, zz, :, yy * TOK : (yy + 1) * TOK] - ls[yy, h : h + 1, :]
                rows = jnp.concatenate(
                    [jnp.broadcast_to(rows[b : b + 1], (BLK, TOK)) for b in range(4)], axis=0
                )
                w = jnp.exp(s[:, lanes] * 0.125 + rows + own * diag_bias)
                d = dp[:, lanes]
                at = yy * 256 + h * TOK
                wf[zz, :, at : at + TOK] = w
                dpf[zz, :, at : at + TOK] = d
                w16[zz, :, at : at + TOK] = w.astype(BF16)
                r = yy * 2 + h
                dl[y, r : r + 1, :] += jnp.sum(w * d, axis=0, keepdims=True)
        return 0

    lax.fori_loop(0, RING, strip, 0)

    for i, off in enumerate(OFFS[1:]):
        send(dl.at[y], dl.at[y], sd.at[i], rd.at[y], along_y(off))

    def value_grad(zz, _):
        dvs[zz] = nn(w16[zz], gm[...].reshape(2048, COLS)).astype(BF16)
        return 0

    lax.fori_loop(0, RING, value_grad, 0)
    for i, off in enumerate(OFFS[1:]):
        send(dvs.at[ring(z, off)], dvr.at[z], sv.at[i], rv.at[z], along_z(off))

    for off in range(1, RING):
        t = ring(tp, off)
        remote(xg.at[t], xg.at[t], sx.at[0], rx.at[t], along_tp(off)).wait_recv()

    def turn(t, _):
        xt[pl.ds(pl.multiple_of(t * 256, 256), 256), :] = xg[t].astype(F32).T.astype(BF16)
        return 0

    lax.fori_loop(0, RING, turn, 0)

    total = dl[y]
    for off in range(1, RING):
        yy = ring(y, off)
        remote(dl.at[yy], dl.at[yy], sd.at[0], rd.at[yy], along_y(off)).wait_recv()
        total = total + dl[yy]

    for yy in range(RING):
        for h in range(2):
            at = yy * 256 + h * TOK
            drow = total[yy * 2 + h : yy * 2 + h + 1, :]

            def score_grad(zz, _, at=at, drow=drow):
                ds16[zz, :, at : at + TOK] = (
                    wf[zz, :, at : at + TOK] * (dpf[zz, :, at : at + TOK] - drow)
                ).astype(BF16)
                return 0

            lax.fori_loop(0, RING, score_grad, 0)

    def query_grad(yy, _):
        lanes0 = pl.ds(pl.multiple_of(yy * 256, 256), 256)
        both = nn(kt[...], ds16[:, :, lanes0].reshape(1024, 256))
        dqs[yy, 0:HD, :] = both[0:HD, 0:TOK].astype(BF16)
        dqs[yy, HD:COLS, :] = both[HD:COLS, TOK:256].astype(BF16)
        return 0

    lax.fori_loop(0, RING, query_grad, 0)
    for i, off in enumerate(OFFS[1:]):
        send(dqs.at[ring(y, off)], dqr.at[y], sdq.at[i], rdq.at[y], along_y(off))

    def key_grad(zz, _):
        dks[zz] = nn(ds16[zz], qm[...].reshape(2048, COLS)).astype(BF16)
        return 0

    lax.fori_loop(0, RING, key_grad, 0)
    for i, off in enumerate(OFFS[1:]):
        send(dks.at[ring(z, off)], dkr.at[z], sdk.at[i], rdk.at[z], along_z(off))

    acc = dqs[y].astype(F32)
    for off in OFFS[1:]:
        yy = ring(y, off)
        remote(dqs.at[yy], dqr.at[yy], sdq.at[0], rdq.at[yy], along_y(off)).wait_recv()
        acc = acc + dqr[yy].astype(F32)
    dq = (acc * 0.125).T.astype(BF16)
    dq_out[...] = dq

    def weight_part(zz, _):
        part = nn(xt[pl.ds(pl.multiple_of(zz * 256, 256), 256), :], dq)
        part = part.astype(BF16).reshape(RING, 2, 16, COLS)
        gas[zz] = part[:, 0]
        gbs[:, zz] = part[:, 1]
        return 0

    lax.fori_loop(0, RING, weight_part, 0)
    for i, off in enumerate(OFFS[1:]):
        send(gas.at[ring(z, off)], gar.at[z], sga.at[i], rga.at[z], along_z(off))
        send(gbs.at[ring(y, off)], gbr.at[y], sgb.at[i], rgb.at[y], along_y(off))

    acc = dvs[z].astype(F32)
    for off in OFFS[1:]:
        zz = ring(z, off)
        remote(dvs.at[zz], dvr.at[zz], sv.at[0], rv.at[zz], along_z(off)).wait_recv()
        acc = acc + dvr[zz].astype(F32)
    dv_out[...] = acc.astype(BF16)

    acc = dks[z].astype(F32)
    for off in OFFS[1:]:
        zz = ring(z, off)
        remote(dks.at[zz], dkr.at[zz], sdk.at[0], rdk.at[zz], along_z(off)).wait_recv()
        acc = acc + dkr[zz].astype(F32)
    dk_out[...] = (acc * 0.125).astype(BF16)

    acc = gas[z].astype(F32)
    for off in OFFS[1:]:
        zz = ring(z, off)
        remote(gas.at[zz], gar.at[zz], sga.at[0], rga.at[zz], along_z(off)).wait_recv()
        acc = acc + gar[zz].astype(F32)
    ha_s[...] = acc.astype(BF16)
    for i, off in enumerate(OFFS[1:]):
        send(ha_s.at[ring(y, off)], ha_r.at[y], sha.at[i], rha.at[y], along_y(off))

    acc = gbs[y].astype(F32)
    for off in OFFS[1:]:
        yy = ring(y, off)
        remote(gbs.at[yy], gbr.at[yy], sgb.at[0], rgb.at[yy], along_y(off)).wait_recv()
        acc = acc + gbr[yy].astype(F32)
    hb_s[...] = acc.astype(BF16)
    for i, off in enumerate(OFFS[1:]):
        send(hb_s.at[ring(z, off)], hb_r.at[z], shb.at[i], rhb.at[z], along_z(off))

    acc = ha_s[y].astype(F32)
    for off in OFFS[1:]:
        yy = ring(y, off)
        remote(ha_s.at[yy], ha_r.at[yy], sha.at[0], rha.at[yy], along_y(off)).wait_recv()
        acc = acc + ha_r[yy].astype(F32)
    gw_out[0:16, :] = acc

    acc = hb_s[z].astype(F32)
    for off in OFFS[1:]:
        zz = ring(z, off)
        remote(hb_s.at[zz], hb_r.at[zz], shb.at[0], rhb.at[zz], along_z(off)).wait_recv()
        acc = acc + hb_r[zz].astype(F32)
    gw_out[16:32, :] = acc

    for c in pending:
        c.wait_send()


def body(queries, keys, values, cotangent, log_sum, chosen, normed_input):
    vm = pltpu.VMEM
    dma = pltpu.SemaphoreType.DMA
    scratch = [
        vm((8, 256, 128), BF16),
        vm((8, 256, 128), BF16),
        vm((8, 2, 128), F32),
        vm((8, 128, 256), BF16),
        vm((2, 32, SEL), jnp.int32),
        vm((8, 256, 128), BF16),
        vm((8, 256, 128), BF16),
        vm((128, 1024), BF16),
        vm((2048, 128), BF16),
        vm((2, 8, 4, 1024), F32),
        vm((8, 128, 2048), F32),
        vm((8, 128, 2048), F32),
        vm((8, 128, 2048), BF16),
        vm((8, 128, 2048), BF16),
        vm((8, 16, 128), F32),
    ]
    scratch += [vm((8, 128, 128), BF16)] * 6
    scratch += [vm((8, 8, 16, 128), BF16)] * 4
    scratch += [vm((8, 16, 128), BF16)] * 4
    scratch += [dma((7,))]
    scratch += [dma((8,))] * 24
    return pl.pallas_call(
        kernel,
        out_shape=(
            jax.ShapeDtypeStruct((TOK, COLS), BF16),
            jax.ShapeDtypeStruct((TOK, COLS), BF16),
            jax.ShapeDtypeStruct((TOK, COLS), BF16),
            jax.ShapeDtypeStruct((32, COLS), F32),
        ),
        in_specs=[pl.BlockSpec(memory_space=pl.ANY)] * 7,
        out_specs=[pl.BlockSpec(memory_space=pltpu.VMEM)] * 4,
        scratch_shapes=scratch,
        compiler_params=pltpu.CompilerParams(
            collective_id=0, has_side_effects=True, vmem_limit_bytes=60 * 1024 * 1024
        ),
    )(queries, keys, values, cotangent, log_sum, chosen, normed_input)


def solution(mesh):
    in_specs = (
        P("kv", "tp"),
        P("kv", "tp"),
        P("kv", "tp"),
        P("kv", "tp"),
        P("tp", "kv"),
        P("tp", None, None),
        P("kv", "tp"),
    )
    out_specs = (P("kv", "tp"), P("kv", "tp"), P("kv", "tp"), P("kv", "tp"))
    return jax.shard_map(body, mesh=mesh, in_specs=in_specs, out_specs=out_specs, check_vma=False)
```

```python
import jax
import jax.numpy as jnp
from jax import lax
from jax.experimental import pallas as pl
from jax.experimental.pallas import tpu as pltpu
from jax.sharding import PartitionSpec as P

HD = 64
BLK = 32
SEL = 12
MASKED = -1e30
RING = 8
TOK = 128
COLS = 128
ORDER = (0, 2, -2, 1, -1, 3, -3, 4)
POS = {off % RING: i for i, off in enumerate(ORDER)}
FAR = (4, 3, -3, 2, -2, 1, -1)
MESH = pl.DeviceIdType.MESH
F32 = jnp.float32
BF16 = jnp.bfloat16


def nt(a, b):
    return lax.dot_general(a, b, (((1,), (1,)), ((), ())), preferred_element_type=F32)


def nn(a, b):
    return lax.dot_general(a, b, (((1,), (0,)), ((), ())), preferred_element_type=F32)


def kernel(
    q_in, k_in, v_in, g_in, ls_in, ch_in, x_in,
    dq_out, dk_out, dv_out, gw_out,
    qg, kv, ls, xg, chs, qm, gm, kt, xt, bias, wf, dpf, w16, ds16, da, dl,
    dvs, dvr, dks, dkr, dqs, dqr, gas, gar, gbs, gbr, ha_s, ha_r, hb_s, hb_r,
    loc, gq, gk, done, come,
):
    me = lax.axis_index("kv")
    tp = lax.axis_index("tp")
    z = me // RING
    y = me % RING

    def ring(base, off):
        return (base + off + RING) % RING

    def along_y(off):
        return (z * RING + ring(y, off), tp)

    def along_z(off):
        return (ring(z, off) * RING + y, tp)

    def along_tp(off):
        return (me, ring(tp, off))

    def remote(src, dst, send, recv, target):
        return pltpu.make_async_remote_copy(
            src_ref=src, dst_ref=dst, send_sem=send, recv_sem=recv, device_id=target, device_id_type=MESH
        )

    def slot(off):
        return POS[off % RING]

    barrier = pltpu.get_barrier_semaphore()
    for off in range(1, RING):
        for target in (along_y(off), along_z(off), along_tp(off)):
            pl.semaphore_signal(barrier, inc=1, device_id=target, device_id_type=MESH)

    first, second = pl.ds(0, TOK), pl.ds(TOK, TOK)
    loads = [
        pltpu.make_async_copy(q_in, qg.at[0, first], loc.at[0]),
        pltpu.make_async_copy(k_in, kv.at[0, first], loc.at[1]),
        pltpu.make_async_copy(g_in, qg.at[0, second], loc.at[2]),
        pltpu.make_async_copy(v_in, kv.at[0, second], loc.at[3]),
        pltpu.make_async_copy(ls_in, ls.at[0], loc.at[4]),
        pltpu.make_async_copy(x_in, xg.at[0], loc.at[5]),
        pltpu.make_async_copy(ch_in, chs, loc.at[6]),
    ]
    for c in loads:
        c.start()
    for c in loads:
        c.wait()
    pl.semaphore_wait(barrier, 3 * (RING - 1))

    halves = (first, second)
    rings = ((qg, along_y, gq, 0), (kv, along_z, gk, 1))
    steps = [(half, r, d) for half in (0, 1) for r in rings for d in (1, -1)]

    def group(off, half):
        near = (off + 4) % RING - 4
        if abs(near) == 2:
            return (0 if near < 0 else 2) + half
        return {1: 4, 3: 5, 4: 6}[abs(near)]

    def pass_on(r, src, half, hop):
        buf, along, sems, n = r
        where = buf.at[slot(src), halves[half]]
        remote(
            where, buf.at[slot(src - hop), halves[half]], done.at[n], sems.at[group(src - hop, half)], along(hop)
        ).start()

    for half, r, d in steps:
        pass_on(r, 0, half, 2 * d)
    for r in rings:
        for d in (1, -1):
            buf, along, sems, n = r
            remote(buf.at[0], buf.at[slot(-d)], done.at[n], sems.at[4], along(d)).start()
    for off in FAR:
        remote(ls.at[0], ls.at[slot(-off)], done.at[2], come.at[2], along_y(off)).start()
    for off in range(1, RING):
        remote(xg.at[0], xg.at[RING - off], done.at[3], come.at[3], along_tp(off)).start()

    lane = lax.broadcasted_iota(jnp.int32, (1, TOK), 1) // BLK
    own_id = jnp.concatenate([(z * RING + ring(y, off)) * 4 + lane for off in ORDER], axis=1)
    spread = (lax.broadcasted_iota(jnp.int32, (256, 1024), 0) == own_id).astype(BF16)
    own_id = own_id.astype(F32)
    lists = [nn(chs[:, h, :].astype(F32).astype(BF16), spread) for h in range(2)]
    for i, off in enumerate(ORDER):
        block = (lax.broadcasted_iota(jnp.int32, (4, 1024), 0) + (ring(z, off) * RING + y) * 4).astype(F32)
        for h in range(2):
            hit = jnp.zeros((4, 1024), F32)
            for s in range(SEL):
                hit = jnp.where(block == lists[h][s : s + 1, :], 1.0, hit)
            hit = jnp.where(block < own_id, hit, 0.0)
            hit = jnp.where(block == own_id, 1.0, hit)
            bias[h, i] = jnp.where(hit > 0.5, 0.0, MASKED)

    head0 = lax.broadcasted_iota(jnp.int32, (TOK, COLS), 1) < HD
    zero = jnp.zeros((TOK, COLS), BF16)

    def stage(i):
        for src, dst in ((first, qm), (second, gm)):
            tile = qg[i, src, :]
            dst[i, first, :] = jnp.where(head0, tile, zero)
            dst[i, second, :] = jnp.where(head0, zero, tile)
        kt[:, i * TOK : (i + 1) * TOK] = kv[i, first, :].astype(F32).T.astype(BF16)

    row_i = lax.broadcasted_iota(jnp.int32, (TOK, TOK), 0)
    col_i = lax.broadcasted_iota(jnp.int32, (TOK, TOK), 1)
    future = (row_i // BLK == col_i // BLK) & (row_i > col_i)
    diag_bias = jnp.where(future, MASKED, 0.0).astype(F32)
    for h in range(2):
        da[h] = jnp.zeros((8, 8, TOK), F32)

    def strip(i, columns, diagonal=False):
        k_tile = kv[i, first, :]
        v_tile = kv[i, second, :]
        for j in columns:
            s = nt(k_tile, qm[j])
            dp = nt(v_tile, gm[j])
            for h in range(2):
                lanes = slice(h * TOK, (h + 1) * TOK)
                rows = bias[h, i, :, j * TOK : (j + 1) * TOK] - ls[j, h : h + 1, :]
                rows = jnp.concatenate(
                    [jnp.broadcast_to(rows[b : b + 1], (BLK, TOK)) for b in range(4)], axis=0
                )
                x = s[:, lanes] * 0.125 + rows
                if diagonal:
                    x = x + diag_bias
                w = jnp.exp(x)
                d = dp[:, lanes]
                at = j * 256 + h * TOK
                wf[i, :, at : at + TOK] = w
                dpf[i, :, at : at + TOK] = d
                w16[i, :, at : at + TOK] = w.astype(BF16)
                da[h, j] += jnp.sum((w * d).reshape(16, 8, TOK), axis=0)

    def strips(lo, hi, columns):
        def one(i, _):
            strip(i, columns)
            return 0

        lax.fori_loop(lo, hi, one, 0)

    stage(0)
    strip(0, (0,), True)

    def wait_group(r, n, ref):
        remote(ref, ref, done.at[r[3]], r[2].at[n], r[1](1)).wait_recv()

    for half, r, d in steps:
        buf = r[0]
        wait_group(r, group(-2 * d, half), buf.at[slot(-2 * d), halves[half]])
        if half == (d < 0):
            pass_on(r, -2 * d, half, 2 * d)
        pass_on(r, -2 * d, half, d)
    remote(ls.at[pl.ds(1, 7)], ls.at[pl.ds(1, 7)], done.at[2], come.at[2], along_y(1)).wait_recv()
    stage(1)
    stage(2)
    strips(1, 3, (0, 1, 2))
    strip(0, (1, 2))
    for r in rings:
        wait_group(r, 4, r[0].at[pl.ds(3, 2)])
    stage(3)
    stage(4)
    strips(3, 5, (0, 1, 2, 3, 4))
    strips(0, 3, (3, 4))
    for r in rings:
        wait_group(r, 5, r[0].at[pl.ds(5, 2)])
    stage(5)
    stage(6)
    strips(5, 7, (0, 1, 2, 3, 4, 5, 6))
    strips(0, 5, (5, 6))
    for r in rings:
        wait_group(r, 6, r[0].at[7])
    stage(7)
    strip(7, (0, 1, 2, 3, 4, 5, 6, 7))
    strips(0, 7, (7,))

    for j, off in enumerate(ORDER):
        for h in range(2):
            dl[0, ring(y, off), h : h + 1, :] = jnp.sum(da[h, j], axis=0, keepdims=True)
    for off in FAR:
        remote(dl.at[0], dl.at[slot(-off)], done.at[4], come.at[4], along_y(off)).start()

    def value_grad(i, _):
        dvs[i] = nn(w16[i], gm[...].reshape(2048, COLS)).astype(BF16)
        return 0

    lax.fori_loop(0, RING, value_grad, 0)
    for off in FAR:
        remote(dvs.at[slot(off)], dvr.at[slot(-off)], done.at[5], come.at[5], along_z(off)).start()

    rest = pl.ds(1, 7)
    remote(xg.at[rest], xg.at[rest], done.at[3], come.at[3], along_tp(1)).wait_recv()
    for o in range(RING):
        xt[pl.ds(pl.multiple_of(ring(tp, o) * 256, 256), 256), :] = xg[o].astype(F32).T.astype(BF16)

    remote(dl.at[rest], dl.at[rest], done.at[4], come.at[4], along_y(1)).wait_recv()

    for off in FAR + (0,):
        j = slot(off)
        total = dl[0, ring(y, off)]
        for n in range(1, RING):
            total = total + dl[n, ring(y, off)]

        def score_grad(i, _, j=j, total=total):
            for h in range(2):
                at = j * 256 + h * TOK
                ds16[i, :, at : at + TOK] = (
                    wf[i, :, at : at + TOK] * (dpf[i, :, at : at + TOK] - total[h : h + 1, :])
                ).astype(BF16)
            return 0

        lax.fori_loop(0, RING, score_grad, 0, unroll=2)
        both = nn(kt[...], ds16[:, :, j * 256 : (j + 1) * 256].reshape(1024, 256))
        dqs[j, 0:HD, :] = both[0:HD, 0:TOK].astype(BF16)
        dqs[j, HD:COLS, :] = both[HD:COLS, TOK:256].astype(BF16)
        if off:
            remote(dqs.at[j], dqr.at[slot(-off)], done.at[6], come.at[6], along_y(off)).start()

    def key_grad(i, _):
        dks[i] = nn(ds16[i], qm[...].reshape(2048, COLS)).astype(BF16)
        return 0

    lax.fori_loop(0, RING, key_grad, 0)
    for off in FAR:
        remote(dks.at[slot(off)], dkr.at[slot(-off)], done.at[7], come.at[7], along_z(off)).start()

    def summed(own, arrived, n, along):
        remote(arrived.at[rest], arrived.at[rest], done.at[n], come.at[n], along(1)).wait_recv()
        acc = own.astype(F32)
        for i in range(1, RING):
            acc = acc + arrived[i].astype(F32)
        return acc

    dq = (summed(dqs[0], dqr, 6, along_y) * 0.125).T.astype(BF16)
    dq_out[...] = dq

    def weight_part(zz, _):
        part = nn(xt[pl.ds(pl.multiple_of(zz * 256, 256), 256), :], dq)
        part = part.astype(BF16).reshape(RING, 2, 16, COLS)
        gas[zz] = part[:, 0]
        gbs[:, zz] = part[:, 1]
        return 0

    lax.fori_loop(0, RING, weight_part, 0)
    for off in FAR:
        remote(gas.at[ring(z, off)], gar.at[slot(-off)], done.at[8], come.at[8], along_z(off)).start()
        remote(gbs.at[ring(y, off)], gbr.at[slot(-off)], done.at[9], come.at[9], along_y(off)).start()

    dv_out[...] = summed(dvs[0], dvr, 5, along_z).astype(BF16)
    dk_out[...] = (summed(dks[0], dkr, 7, along_z) * 0.125).astype(BF16)

    ha_s[...] = summed(gas[z], gar, 8, along_z).astype(BF16)
    for off in FAR:
        remote(ha_s.at[ring(y, off)], ha_r.at[slot(-off)], done.at[10], come.at[10], along_y(off)).start()
    hb_s[...] = summed(gbs[y], gbr, 9, along_y).astype(BF16)
    for off in FAR:
        remote(hb_s.at[ring(z, off)], hb_r.at[slot(-off)], done.at[11], come.at[11], along_z(off)).start()
    gw_out[0:16, :] = summed(ha_s[y], ha_r, 10, along_y)
    gw_out[16:32, :] = summed(hb_s[z], hb_r, 11, along_z)

    for n, ref in enumerate((qg, kv, ls, xg, dl, dvs, dqs, dks, gas, gbs, ha_s, hb_s)):
        part = ref.at[rest]
        remote(part, part, done.at[n], come.at[n], along_y(1)).wait_send()


def body(queries, keys, values, cotangent, log_sum, chosen, normed_input):
    vm = pltpu.VMEM
    dma = pltpu.SemaphoreType.DMA
    scratch = [
        vm((8, 256, 128), BF16),
        vm((8, 256, 128), BF16),
        vm((8, 2, 128), F32),
        vm((8, 128, 256), BF16),
        vm((SEL, 2, 256), jnp.int32),
        vm((8, 256, 128), BF16),
        vm((8, 256, 128), BF16),
        vm((128, 1024), BF16),
        vm((2048, 128), BF16),
        vm((2, 8, 4, 1024), F32),
        vm((8, 128, 2048), F32),
        vm((8, 128, 2048), F32),
        vm((8, 128, 2048), BF16),
        vm((8, 128, 2048), BF16),
        vm((2, 8, 8, 128), F32),
        vm((8, 8, 2, 128), F32),
    ]
    scratch += [vm((8, 128, 128), BF16)] * 6
    scratch += [vm((8, 8, 16, 128), BF16)] * 4
    scratch += [vm((8, 16, 128), BF16)] * 4
    scratch += [dma((7,)), dma((7,)), dma((7,)), dma((12,)), dma((12,))]
    return pl.pallas_call(
        kernel,
        out_shape=(
            jax.ShapeDtypeStruct((TOK, COLS), BF16),
            jax.ShapeDtypeStruct((TOK, COLS), BF16),
            jax.ShapeDtypeStruct((TOK, COLS), BF16),
            jax.ShapeDtypeStruct((32, COLS), F32),
        ),
        in_specs=[pl.BlockSpec(memory_space=pl.ANY)] * 7,
        out_specs=[pl.BlockSpec(memory_space=pltpu.VMEM)] * 4,
        scratch_shapes=scratch,
        compiler_params=pltpu.CompilerParams(
            collective_id=0, has_side_effects=True, vmem_limit_bytes=60 * 1024 * 1024
        ),
    )(queries, keys, values, cotangent, log_sum, chosen.transpose(2, 0, 1), normed_input)


def solution(mesh):
    in_specs = (
        P("kv", "tp"),
        P("kv", "tp"),
        P("kv", "tp"),
        P("kv", "tp"),
        P("tp", "kv"),
        P("tp", None, None),
        P("kv", "tp"),
    )
    out_specs = (P("kv", "tp"), P("kv", "tp"), P("kv", "tp"), P("kv", "tp"))
    return jax.shard_map(body, mesh=mesh, in_specs=in_specs, out_specs=out_specs, check_vma=False)
```

```python
import jax
import jax.numpy as jnp
from jax import lax
from jax.experimental import pallas as pl
from jax.experimental.pallas import tpu as pltpu
from jax.sharding import PartitionSpec as P

HD = 64
BLK = 32
SEL = 12
MASKED = -1e30
RING = 8
TOK = 128
COLS = 128
ORDER = (0, 2, -2, 1, -1, 3, -3, 4)
POS = {off % RING: i for i, off in enumerate(ORDER)}
FAR = (4, 3, -3, 2, -2, 1, -1)
MESH = pl.DeviceIdType.MESH
F32 = jnp.float32
BF16 = jnp.bfloat16


def nt(a, b):
    return lax.dot_general(a, b, (((1,), (1,)), ((), ())), preferred_element_type=F32)


def nn(a, b):
    return lax.dot_general(a, b, (((1,), (0,)), ((), ())), preferred_element_type=F32)


def kernel(
    q_in, k_in, v_in, g_in, ls_in, ch_in, x_in,
    dq_out, dk_out, dv_out, gw_out,
    raw, qg, kv, ls, xg, chs, qmt, gmt, kt, xt, bias, wf, dpf, w16, ds16, da, dl, tot,
    dvs, dvr, dks, dkr, dqs, dqr, gas, gar, gbs, gbr, ha_s, ha_r, hb_s, hb_r,
    loc, gather, done, come,
):
    me = lax.axis_index("kv")
    tp = lax.axis_index("tp")
    z = me // RING
    y = me % RING

    def ring(base, off):
        return (base + off + RING) % RING

    def dev(axis, off):
        return z * RING + ring(y, off) if axis == 0 else ring(z, off) * RING + y

    def along(axis, off):
        return (dev(axis, off), tp)

    def remote(src, dst, send, recv, target):
        return pltpu.make_async_remote_copy(
            src_ref=src, dst_ref=dst, send_sem=send, recv_sem=recv, device_id=target, device_id_type=MESH
        )

    def slot(off):
        return POS[off % RING]

    barrier = pltpu.get_barrier_semaphore()
    for off in range(1, RING):
        for target in (along(0, off), along(1, off), (me, ring(tp, off))):
            pl.semaphore_signal(barrier, inc=1, device_id=target, device_id_type=MESH)

    loads = [
        pltpu.make_async_copy(src, dst, loc.at[n])
        for n, (src, dst) in enumerate(
            (
                (q_in, raw.at[0]), (g_in, raw.at[1]), (k_in, raw.at[2]), (v_in, raw.at[3]),
                (ls_in, ls.at[0, 0]), (ls_in, ls.at[1, 0]), (x_in, xg.at[0]), (ch_in, chs),
            )
        )
    ]
    for c in loads:
        c.start()
    left = lax.broadcasted_iota(jnp.int32, (TOK, COLS), 1) < HD
    for n, buf in ((0, qg), (2, kv)):
        loads[n].wait()
        loads[n + 1].wait()
        a, b = raw[n].astype(F32), raw[n + 1].astype(F32)
        buf[0, 0] = jnp.where(left, a, pltpu.roll(b, HD, 1)).astype(BF16)
        buf[1, 0] = jnp.where(left, pltpu.roll(a, HD, 1), b).astype(BF16)
    for c in loads[4:]:
        c.wait()
    pl.semaphore_wait(barrier, 3 * (RING - 1))

    def piece(axis, half):
        return qg.at[axis] if half == 0 else kv.at[1 - axis]

    steps = [(half, axis, d) for half in (0, 1) for axis in (0, 1) for d in (1, -1)]

    def group(off, half):
        near = (off + 4) % RING - 4
        if abs(near) == 2:
            return (0 if near < 0 else 2) + half
        return {1: 4, 3: 6, 4: 8}[abs(near)] + half

    def pass_on(axis, src, half, hop):
        buf = piece(axis, half)
        remote(
            buf.at[slot(src)],
            buf.at[slot(src - hop)],
            done.at[2 * axis + half],
            gather.at[axis, group(src - hop, half)],
            along(axis, hop),
        ).start()

    for half, axis, d in steps:
        pass_on(axis, 0, half, 2 * d)
    for half, axis, d in steps:
        pass_on(axis, 0, half, d)
    for off in FAR:
        for axis in (0, 1):
            remote(
                ls.at[axis, 0], ls.at[axis, slot(-off)], done.at[4 + axis], come.at[4 + axis], along(axis, off)
            ).start()
    for off in range(1, RING):
        remote(xg.at[0], xg.at[RING - off], done.at[6], come.at[6], (me, ring(tp, off))).start()

    lane = lax.broadcasted_iota(jnp.int32, (1, TOK), 1) // BLK
    for h in range(2):
        own_id = jnp.concatenate([dev(h, off) * 4 + lane for off in ORDER], axis=1)
        spread = (lax.broadcasted_iota(jnp.int32, (256, 1024), 0) == own_id).astype(BF16)
        own_id = own_id.astype(F32)
        lists = nn(chs[:, h, :].astype(F32).astype(BF16), spread)
        for i, off in enumerate(ORDER):
            block = (lax.broadcasted_iota(jnp.int32, (4, 1024), 0) + dev(1 - h, off) * 4).astype(F32)
            hit = jnp.zeros((4, 1024), F32)
            for s in range(SEL):
                hit = jnp.where(block == lists[s : s + 1, :], 1.0, hit)
            hit = jnp.where(block < own_id, hit, 0.0)
            hit = jnp.where(block == own_id, 1.0, hit)
            bias[h, i] = jnp.where(hit > 0.5, 0.0, MASKED)

    for h in range(2):
        qmt[h, HD:COLS, :] = jnp.zeros((HD, 1024), BF16)
        gmt[h, 0:HD, :] = jnp.zeros((HD, 1024), BF16)
        da[h] = jnp.zeros((8, 8, TOK), F32)

    def stage(i):
        lanes = slice(i * TOK, (i + 1) * TOK)
        for h in range(2):
            turned = qg[h, i].astype(F32).T.astype(BF16)
            qmt[h, 0:HD, lanes] = turned[0:HD]
            gmt[h, HD:COLS, lanes] = turned[HD:COLS]
            kt[h, :, lanes] = kv[h, i].astype(F32).T[0:HD].astype(BF16)

    row_i = lax.broadcasted_iota(jnp.int32, (TOK, TOK), 0)
    col_i = lax.broadcasted_iota(jnp.int32, (TOK, TOK), 1)
    future = (row_i // BLK == col_i // BLK) & (row_i > col_i)
    diag_bias = jnp.where(future, MASKED, 0.0).astype(F32)

    def strip(i, lo, hi, diagonal=False):
        for h in range(2):
            tile = kv[h, i]
            for at in range(lo, hi, 2):
                end = min(at + 2, hi)
                s = nn(tile, qmt[h, :, at * TOK : end * TOK])
                dp = nn(tile, gmt[h, :, at * TOK : end * TOK])
                for j in range(at, end):
                    lanes = slice((j - at) * TOK, (j - at + 1) * TOK)
                    into = slice(j * TOK, (j + 1) * TOK)
                    rows = bias[h, i, :, into] - ls[h, j, h : h + 1, :]
                    rows = jnp.concatenate(
                        [jnp.broadcast_to(rows[b : b + 1], (BLK, TOK)) for b in range(4)], axis=0
                    )
                    x = s[:, lanes] * 0.125 + rows
                    if diagonal:
                        x = x + diag_bias
                    w = jnp.exp(x)
                    d = dp[:, lanes]
                    wf[h, i, :, into] = w
                    dpf[h, i, :, into] = d
                    w16[h, i, :, into] = w.astype(BF16)
                    da[h, j] += jnp.sum((w * d).reshape(16, 8, TOK), axis=0)

    def strips(first, last, lo, hi, unroll=1):
        def one(i, _):
            strip(i, lo, hi)
            return 0

        lax.fori_loop(first, last, one, 0, unroll=unroll)

    stage(0)
    strip(0, 0, 1, True)

    def arrive(axis, n, ref):
        remote(ref, ref, done.at[2 * axis], gather.at[axis, n], along(axis, 1)).wait_recv()

    rest = pl.ds(1, 7)
    for half, axis, d in steps:
        arrive(axis, group(-2 * d, half), piece(axis, half).at[slot(-2 * d)])
        if half == (d < 0):
            pass_on(axis, -2 * d, half, 2 * d)
        pass_on(axis, -2 * d, half, d)
    for axis in (0, 1):
        part = ls.at[axis, rest]
        remote(part, part, done.at[4 + axis], come.at[4 + axis], along(axis, 1)).wait_recv()
    stage(1)
    stage(2)
    strips(1, 3, 0, 3)
    strip(0, 1, 3)
    for n, first in ((4, 3), (6, 5)):
        for axis in (0, 1):
            for half in (0, 1):
                arrive(axis, n + half, piece(axis, half).at[pl.ds(first, 2)])
        stage(first)
        stage(first + 1)
        strips(first, first + 2, 0, first + 2)
        strips(0, first, first, first + 2)
    for axis in (0, 1):
        for half in (0, 1):
            arrive(axis, 8 + half, piece(axis, half).at[7])
    stage(7)
    strip(7, 0, 8)
    strips(0, 7, 7, 8, unroll=7)

    for axis in (0, 1):
        for j, off in enumerate(ORDER):
            row = ring(y if axis == 0 else z, off)
            dl[axis, 0, pl.ds(row, 1), :] = jnp.sum(da[axis, j], axis=0, keepdims=True)
    for off in FAR:
        for axis in (0, 1):
            remote(
                dl.at[axis, 0], dl.at[axis, slot(-off)], done.at[7 + axis], come.at[7 + axis], along(axis, off)
            ).start()

    def scatter(buf, into, h, axis, n):
        for off in FAR:
            remote(
                buf.at[h, slot(off)], into.at[h, slot(-off)], done.at[n + h], come.at[n + h], along(axis, off)
            ).start()

    def value_grad(i, _):
        for h in range(2):
            dvs[h, i] = nt(gmt[h, HD:COLS, :], w16[h, i]).astype(BF16)
        return 0

    lax.fori_loop(0, RING, value_grad, 0)
    for h in range(2):
        scatter(dvs, dvr, h, 1 - h, 9)

    part = xg.at[rest]
    remote(part, part, done.at[6], come.at[6], (me, ring(tp, 1))).wait_recv()
    for o in range(RING):
        xt[pl.ds(pl.multiple_of(ring(tp, o) * 256, 256), 256), :] = xg[o].astype(F32).T.astype(BF16)

    for axis in (0, 1):
        part = dl.at[axis, rest]
        remote(part, part, done.at[7 + axis], come.at[7 + axis], along(axis, 1)).wait_recv()
        acc = dl[axis, 0]
        for n in range(1, RING):
            acc = acc + dl[axis, n]
        tot[axis] = acc

    for off in FAR + (0,):
        j = slot(off)
        into = slice(j * TOK, (j + 1) * TOK)
        for h in range(2):
            delta = tot[h, pl.ds(ring(y if h == 0 else z, off), 1), :]

            def score_grad(i, _, h=h, into=into, delta=delta):
                ds16[h, i, :, into] = (wf[h, i, :, into] * (dpf[h, i, :, into] - delta)).astype(BF16)
                return 0

            lax.fori_loop(0, RING, score_grad, 0, unroll=4)
            dqs[h, j] = nn(kt[h], ds16[h, :, :, into].reshape(1024, TOK)).astype(BF16)
            if off:
                remote(
                    dqs.at[h, j], dqr.at[h, slot(-off)], done.at[11 + h], come.at[11 + h], along(h, off)
                ).start()

    def key_grad(i, _):
        for h in range(2):
            dks[h, i] = nt(qmt[h, 0:HD, :], ds16[h, i]).astype(BF16)
        return 0

    lax.fori_loop(0, RING, key_grad, 0)
    for h in range(2):
        scatter(dks, dkr, h, 1 - h, 13)

    def both_heads(own, arrived, n):
        sums = []
        for h in range(2):
            part = arrived.at[h, rest]
            remote(part, part, done.at[n + h], come.at[n + h], along(0, 1)).wait_recv()
            acc = own[h, 0].astype(F32)
            for i in range(1, RING):
                acc = acc + arrived[h, i].astype(F32)
            sums.append(acc)
        return jnp.concatenate(sums, axis=0).T

    dq = (both_heads(dqs, dqr, 11) * 0.125).astype(BF16)
    dq_out[...] = dq

    def weight_part(zz, _):
        part = nn(xt[pl.ds(pl.multiple_of(zz * 256, 256), 256), :], dq)
        part = part.astype(BF16).reshape(RING, 2, 16, COLS)
        gas[zz] = part[:, 0]
        gbs[:, zz] = part[:, 1]
        return 0

    lax.fori_loop(0, RING, weight_part, 0, unroll=4)
    for off in FAR:
        remote(gas.at[ring(z, off)], gar.at[slot(-off)], done.at[15], come.at[15], along(1, off)).start()
        remote(gbs.at[ring(y, off)], gbr.at[slot(-off)], done.at[16], come.at[16], along(0, off)).start()

    dv_out[...] = both_heads(dvs, dvr, 9).astype(BF16)
    dk_out[...] = (both_heads(dks, dkr, 13) * 0.125).astype(BF16)

    def summed(own, arrived, n):
        part = arrived.at[rest]
        remote(part, part, done.at[n], come.at[n], along(0, 1)).wait_recv()
        acc = own.astype(F32)
        for i in range(1, RING):
            acc = acc + arrived[i].astype(F32)
        return acc

    ha_s[...] = summed(gas[z], gar, 15).astype(BF16)
    for off in FAR:
        remote(ha_s.at[ring(y, off)], ha_r.at[slot(-off)], done.at[17], come.at[17], along(0, off)).start()
    hb_s[...] = summed(gbs[y], gbr, 16).astype(BF16)
    for off in FAR:
        remote(hb_s.at[ring(z, off)], hb_r.at[slot(-off)], done.at[18], come.at[18], along(1, off)).start()
    gw_out[0:16, :] = summed(ha_s[y], ha_r, 17)
    gw_out[16:32, :] = summed(hb_s[z], hb_r, 18)

    sent = [qg.at[0, rest], kv.at[1, rest], qg.at[1, rest], kv.at[0, rest], ls.at[0, rest], ls.at[1, rest]]
    sent += [xg.at[rest], dl.at[0, rest], dl.at[1, rest]]
    sent += [buf.at[h, rest] for buf in (dvs, dqs, dks) for h in range(2)]
    sent += [buf.at[rest] for buf in (gas, gbs, ha_s, hb_s)]
    for n, part in enumerate(sent):
        remote(part, part, done.at[n], come.at[n], along(0, 1)).wait_send()


def write_out(a, b, c, d, a_out, b_out, c_out, d_out, sems):
    copies = [
        pltpu.make_async_copy(src, dst, sems.at[n])
        for n, (src, dst) in enumerate(((a, a_out), (b, b_out), (c, c_out), (d, d_out)))
    ]
    for copy in copies:
        copy.start()
    for copy in copies:
        copy.wait()


def body(queries, keys, values, cotangent, log_sum, chosen, normed_input):
    vm = pltpu.VMEM
    dma = pltpu.SemaphoreType.DMA
    scratch = [
        vm((4, 128, 128), BF16),
        vm((2, 8, 128, 128), BF16),
        vm((2, 8, 128, 128), BF16),
        vm((2, 8, 2, 128), F32),
        vm((8, 128, 256), BF16),
        vm((SEL, 2, 256), jnp.int32),
        vm((2, 128, 1024), BF16),
        vm((2, 128, 1024), BF16),
        vm((2, 64, 1024), BF16),
        vm((2048, 128), BF16),
        vm((2, 8, 4, 1024), F32),
        vm((2, 8, 128, 1024), F32),
        vm((2, 8, 128, 1024), F32),
        vm((2, 8, 128, 1024), BF16),
        vm((2, 8, 128, 1024), BF16),
        vm((2, 8, 8, 128), F32),
        vm((2, 8, 8, 128), F32),
        vm((2, 8, 128), F32),
    ]
    scratch += [vm((2, 8, 64, 128), BF16)] * 6
    scratch += [vm((8, 8, 16, 128), BF16)] * 4
    scratch += [vm((8, 16, 128), BF16)] * 4
    scratch += [dma((8,)), dma((2, 10)), dma((19,)), dma((19,))]
    shapes = (
        jax.ShapeDtypeStruct((TOK, COLS), BF16),
        jax.ShapeDtypeStruct((TOK, COLS), BF16),
        jax.ShapeDtypeStruct((TOK, COLS), BF16),
        jax.ShapeDtypeStruct((32, COLS), F32),
    )
    inside = pl.pallas_call(
        kernel,
        out_shape=shapes,
        in_specs=[pl.BlockSpec(memory_space=pl.ANY)] * 7,
        out_specs=[pl.BlockSpec(memory_space=pltpu.VMEM)] * 4,
        scratch_shapes=scratch,
        compiler_params=pltpu.CompilerParams(
            collective_id=0, has_side_effects=True, vmem_limit_bytes=55080 * 1024
        ),
    )(queries, keys, values, cotangent, log_sum, chosen.transpose(2, 0, 1), normed_input)
    return pl.pallas_call(
        write_out,
        out_shape=shapes,
        in_specs=[pl.BlockSpec(memory_space=pltpu.VMEM)] * 4,
        out_specs=[pl.BlockSpec(memory_space=pl.ANY)] * 4,
        scratch_shapes=[dma((4,))],
        compiler_params=pltpu.CompilerParams(vmem_limit_bytes=4 * 1024 * 1024),
    )(*inside)


def solution(mesh):
    in_specs = (
        P("kv", "tp"),
        P("kv", "tp"),
        P("kv", "tp"),
        P("kv", "tp"),
        P("tp", "kv"),
        P("tp", None, None),
        P("kv", "tp"),
    )
    out_specs = (P("kv", "tp"), P("kv", "tp"), P("kv", "tp"), P("kv", "tp"))
    return jax.shard_map(body, mesh=mesh, in_specs=in_specs, out_specs=out_specs, check_vma=False)
```

```python
import jax
import jax.numpy as jnp
from jax import lax
from jax.experimental import pallas as pl
from jax.experimental.pallas import tpu as pltpu
from jax.sharding import PartitionSpec as P

HD = 64
BLK = 32
SEL = 12
MASKED = -1e30
RING = 8
TOK = 128
COLS = 128
ORDER = (0, 2, -2, 1, -1, 3, -3, 4)
POS = {off % RING: i for i, off in enumerate(ORDER)}
FAR = (4, 3, -3, 2, -2, 1, -1)
MESH = pl.DeviceIdType.MESH
F32 = jnp.float32
BF16 = jnp.bfloat16


def nt(a, b):
    return lax.dot_general(a, b, (((1,), (1,)), ((), ())), preferred_element_type=F32)


def nn(a, b):
    return lax.dot_general(a, b, (((1,), (0,)), ((), ())), preferred_element_type=F32)


def kernel(
    q_in, k_in, v_in, g_in, ls_in, ch_in, x_in,
    dq_out, dk_out, dv_out, gw_out,
    raw, qg, kv, ls, xg, chs, qmt, gmt, kt, xt, bias, wf, dpf, w16, ds16, da, dl, tot,
    dvs, dvr, dks, dkr, dqs, dqr, gas, gar, gbs, gbr, ha_s, ha_r, hb_s, hb_r,
    loc, gather, done, come,
):
    me = lax.axis_index("kv")
    tp = lax.axis_index("tp")
    z = me // RING
    y = me % RING

    def ring(base, off):
        return (base + off + RING) % RING

    def dev(axis, off):
        return z * RING + ring(y, off) if axis == 0 else ring(z, off) * RING + y

    def along(axis, off):
        return (dev(axis, off), tp)

    def remote(src, dst, send, recv, target):
        return pltpu.make_async_remote_copy(
            src_ref=src, dst_ref=dst, send_sem=send, recv_sem=recv, device_id=target, device_id_type=MESH
        )

    def slot(off):
        return POS[off % RING]

    barrier = pltpu.get_barrier_semaphore()
    for off in range(1, RING):
        for target in (along(0, off), along(1, off), (me, ring(tp, off))):
            pl.semaphore_signal(barrier, inc=1, device_id=target, device_id_type=MESH)

    loads = [
        pltpu.make_async_copy(src, dst, loc.at[n])
        for n, (src, dst) in enumerate(
            (
                (q_in, raw.at[0]), (g_in, raw.at[1]), (k_in, raw.at[2]), (v_in, raw.at[3]),
                (ls_in, ls.at[0, 0]), (ls_in, ls.at[1, 0]), (x_in, xg.at[0]), (ch_in, chs),
            )
        )
    ]
    for c in loads:
        c.start()
    left = lax.broadcasted_iota(jnp.int32, (TOK, COLS), 1) < HD
    for n, buf in ((0, qg), (2, kv)):
        loads[n].wait()
        loads[n + 1].wait()
        a, b = raw[n].astype(F32), raw[n + 1].astype(F32)
        buf[0, 0] = jnp.where(left, a, pltpu.roll(b, HD, 1)).astype(BF16)
        buf[1, 0] = jnp.where(left, pltpu.roll(a, HD, 1), b).astype(BF16)
    for c in loads[4:]:
        c.wait()
    pl.semaphore_wait(barrier, 3 * (RING - 1))

    def piece(axis, half):
        return qg.at[axis] if half == 0 else kv.at[1 - axis]

    steps = [(half, axis, d) for half in (0, 1) for axis in (0, 1) for d in (1, -1)]

    def group(off, half):
        near = (off + 4) % RING - 4
        if abs(near) == 2:
            return (0 if near < 0 else 2) + half
        return {1: 4, 3: 6, 4: 8}[abs(near)] + half

    def pass_on(axis, src, half, hop):
        buf = piece(axis, half)
        remote(
            buf.at[slot(src)],
            buf.at[slot(src - hop)],
            done.at[2 * axis + half],
            gather.at[axis, group(src - hop, half)],
            along(axis, hop),
        ).start()

    for half, axis, d in steps:
        pass_on(axis, 0, half, 2 * d)
    for half, axis, d in steps:
        pass_on(axis, 0, half, d)
    for off in FAR:
        for axis in (0, 1):
            remote(
                ls.at[axis, 0], ls.at[axis, slot(-off)], done.at[4 + axis], come.at[4 + axis], along(axis, off)
            ).start()
    for off in range(1, RING):
        remote(xg.at[0], xg.at[RING - off], done.at[6], come.at[6], (me, ring(tp, off))).start()

    lane = lax.broadcasted_iota(jnp.int32, (1, TOK), 1) // BLK
    for h in range(2):
        own_id = jnp.concatenate([dev(h, off) * 4 + lane for off in ORDER], axis=1)
        spread = (lax.broadcasted_iota(jnp.int32, (256, 1024), 0) == own_id).astype(BF16)
        own_id = own_id.astype(F32)
        lists = nn(chs[:, h, :].astype(F32).astype(BF16), spread)
        for i, off in enumerate(ORDER):
            block = (lax.broadcasted_iota(jnp.int32, (4, 1024), 0) + dev(1 - h, off) * 4).astype(F32)
            hit = jnp.zeros((4, 1024), F32)
            for s in range(SEL):
                hit = jnp.where(block == lists[s : s + 1, :], 1.0, hit)
            hit = jnp.where(block < own_id, hit, 0.0)
            hit = jnp.where(block == own_id, 1.0, hit)
            bias[h, i] = jnp.where(hit > 0.5, 0.0, MASKED)

    for h in range(2):
        qmt[h, HD:COLS, :] = jnp.zeros((HD, 1024), BF16)
        gmt[h, 0:HD, :] = jnp.zeros((HD, 1024), BF16)
        da[h] = jnp.zeros((8, 8, TOK), F32)

    def stage(i):
        lanes = slice(i * TOK, (i + 1) * TOK)
        for h in range(2):
            turned = qg[h, i].astype(F32).T.astype(BF16)
            qmt[h, 0:HD, lanes] = turned[0:HD]
            gmt[h, HD:COLS, lanes] = turned[HD:COLS]
            kt[h, :, lanes] = kv[h, i].astype(F32).T[0:HD].astype(BF16)

    row_i = lax.broadcasted_iota(jnp.int32, (TOK, TOK), 0)
    col_i = lax.broadcasted_iota(jnp.int32, (TOK, TOK), 1)
    future = (row_i // BLK == col_i // BLK) & (row_i > col_i)
    diag_bias = jnp.where(future, MASKED, 0.0).astype(F32)

    def strip(i, lo, hi, diagonal=False):
        for h in range(2):
            tile = kv[h, i]
            for at in range(lo, hi, 2):
                end = min(at + 2, hi)
                s = nn(tile, qmt[h, :, at * TOK : end * TOK])
                dp = nn(tile, gmt[h, :, at * TOK : end * TOK])
                for j in range(at, end):
                    lanes = slice((j - at) * TOK, (j - at + 1) * TOK)
                    into = slice(j * TOK, (j + 1) * TOK)
                    rows = bias[h, i, :, into] - ls[h, j, h : h + 1, :]
                    rows = jnp.concatenate(
                        [jnp.broadcast_to(rows[b : b + 1], (BLK, TOK)) for b in range(4)], axis=0
                    )
                    x = s[:, lanes] * 0.125 + rows
                    if diagonal:
                        x = x + diag_bias
                    w = jnp.exp(x)
                    d = dp[:, lanes]
                    wf[h, i, :, into] = w
                    dpf[h, i, :, into] = d
                    w16[h, i, :, into] = w.astype(BF16)
                    da[h, j] += jnp.sum((w * d).reshape(16, 8, TOK), axis=0)

    def strips(first, last, lo, hi, unroll=1):
        def one(i, _):
            strip(i, lo, hi)
            return 0

        lax.fori_loop(first, last, one, 0, unroll=unroll)

    stage(0)
    strip(0, 0, 1, True)

    def arrive(axis, n, ref):
        remote(ref, ref, done.at[2 * axis], gather.at[axis, n], along(axis, 1)).wait_recv()

    rest = pl.ds(1, 7)
    for half, axis, d in steps:
        arrive(axis, group(-2 * d, half), piece(axis, half).at[slot(-2 * d)])
        if half == (d < 0):
            pass_on(axis, -2 * d, half, 2 * d)
        pass_on(axis, -2 * d, half, d)
    for axis in (0, 1):
        part = ls.at[axis, rest]
        remote(part, part, done.at[4 + axis], come.at[4 + axis], along(axis, 1)).wait_recv()
    stage(1)
    stage(2)
    strips(1, 3, 0, 3)
    strip(0, 1, 3)
    for n, first in ((4, 3), (6, 5)):
        for axis in (0, 1):
            for half in (0, 1):
                arrive(axis, n + half, piece(axis, half).at[pl.ds(first, 2)])
        stage(first)
        stage(first + 1)
        strips(first, first + 2, 0, first + 2)
        strips(0, first, first, first + 2)
    for axis in (0, 1):
        for half in (0, 1):
            arrive(axis, 8 + half, piece(axis, half).at[7])
    stage(7)
    strip(7, 0, 8)
    strips(0, 7, 7, 8, unroll=7)

    for axis in (0, 1):
        for j, off in enumerate(ORDER):
            row = ring(y if axis == 0 else z, off)
            dl[axis, 0, pl.ds(row, 1), :] = jnp.sum(da[axis, j], axis=0, keepdims=True)
    for off in FAR:
        for axis in (0, 1):
            remote(
                dl.at[axis, 0], dl.at[axis, slot(-off)], done.at[7 + axis], come.at[7 + axis], along(axis, off)
            ).start()

    def scatter(buf, into, h, axis, n):
        for off in FAR:
            remote(
                buf.at[h, slot(off)], into.at[h, slot(-off)], done.at[n + h], come.at[n + h], along(axis, off)
            ).start()

    def value_grad(i, _):
        for h in range(2):
            dvs[h, i] = nt(gmt[h, HD:COLS, :], w16[h, i]).astype(BF16)
        return 0

    lax.fori_loop(0, RING, value_grad, 0, unroll=4)
    for h in range(2):
        scatter(dvs, dvr, h, 1 - h, 9)

    part = xg.at[rest]
    remote(part, part, done.at[6], come.at[6], (me, ring(tp, 1))).wait_recv()
    for o in range(RING):
        xt[pl.ds(pl.multiple_of(ring(tp, o) * 256, 256), 256), :] = xg[o].astype(F32).T.astype(BF16)

    for axis in (0, 1):
        part = dl.at[axis, rest]
        remote(part, part, done.at[7 + axis], come.at[7 + axis], along(axis, 1)).wait_recv()
        acc = dl[axis, 0]
        for n in range(1, RING):
            acc = acc + dl[axis, n]
        tot[axis] = acc

    for lo, hi in ((7, 8), (5, 7), (1, 3), (3, 5), (0, 1)):
        into = slice(lo * TOK, hi * TOK)
        for h in range(2):
            delta = jnp.concatenate(
                [tot[h, pl.ds(ring(y if h == 0 else z, ORDER[j]), 1), :] for j in range(lo, hi)], axis=1
            )
            acc = jnp.zeros((HD, (hi - lo) * TOK), F32)
            for i in range(0, RING, 2):
                pair = []
                for n in (i, i + 1):
                    low = (wf[h, n, :, into] * (dpf[h, n, :, into] - delta)).astype(BF16)
                    ds16[h, n, :, into] = low
                    pair.append(low)
                acc = acc + nn(kt[h, :, i * TOK : (i + 2) * TOK], jnp.concatenate(pair, axis=0))
            for j in range(lo, hi):
                dqs[h, j] = acc[:, (j - lo) * TOK : (j - lo + 1) * TOK].astype(BF16)
        for j in range(max(lo, 1), hi):
            for h in range(2):
                remote(
                    dqs.at[h, j], dqr.at[h, slot(-ORDER[j])], done.at[11 + h], come.at[11 + h], along(h, ORDER[j])
                ).start()

    def key_grad(i, _):
        for h in range(2):
            dks[h, i] = nt(qmt[h, 0:HD, :], ds16[h, i]).astype(BF16)
        return 0

    lax.fori_loop(0, RING, key_grad, 0, unroll=4)
    for h in range(2):
        scatter(dks, dkr, h, 1 - h, 13)

    def both_heads(own, arrived, n):
        sums = []
        for h in range(2):
            part = arrived.at[h, rest]
            remote(part, part, done.at[n + h], come.at[n + h], along(0, 1)).wait_recv()
            acc = own[h, 0].astype(F32)
            for i in range(1, RING):
                acc = acc + arrived[h, i].astype(F32)
            sums.append(acc)
        return jnp.concatenate(sums, axis=0).T

    dq = (both_heads(dqs, dqr, 11) * 0.125).astype(BF16)
    dq_out[...] = dq

    def weight_part(zz, _):
        part = nn(xt[pl.ds(pl.multiple_of(zz * 256, 256), 256), :], dq)
        part = part.astype(BF16).reshape(RING, 2, 16, COLS)
        gas[zz] = part[:, 0]
        gbs[:, zz] = part[:, 1]
        return 0

    lax.fori_loop(0, RING, weight_part, 0, unroll=4)
    for off in FAR:
        remote(gas.at[ring(z, off)], gar.at[slot(-off)], done.at[15], come.at[15], along(1, off)).start()
        remote(gbs.at[ring(y, off)], gbr.at[slot(-off)], done.at[16], come.at[16], along(0, off)).start()

    dv_out[...] = both_heads(dvs, dvr, 9).astype(BF16)
    dk_out[...] = (both_heads(dks, dkr, 13) * 0.125).astype(BF16)

    def summed(own, arrived, n):
        part = arrived.at[rest]
        remote(part, part, done.at[n], come.at[n], along(0, 1)).wait_recv()
        acc = own.astype(F32)
        for i in range(1, RING):
            acc = acc + arrived[i].astype(F32)
        return acc

    ha_s[...] = summed(gas[z], gar, 15).astype(BF16)
    for off in FAR:
        remote(ha_s.at[ring(y, off)], ha_r.at[slot(-off)], done.at[17], come.at[17], along(0, off)).start()
    hb_s[...] = summed(gbs[y], gbr, 16).astype(BF16)
    for off in FAR:
        remote(hb_s.at[ring(z, off)], hb_r.at[slot(-off)], done.at[18], come.at[18], along(1, off)).start()
    gw_out[0:16, :] = summed(ha_s[y], ha_r, 17)
    gw_out[16:32, :] = summed(hb_s[z], hb_r, 18)

    sent = [qg.at[0, rest], kv.at[1, rest], qg.at[1, rest], kv.at[0, rest], ls.at[0, rest], ls.at[1, rest]]
    sent += [xg.at[rest], dl.at[0, rest], dl.at[1, rest]]
    sent += [buf.at[h, rest] for buf in (dvs, dqs, dks) for h in range(2)]
    sent += [buf.at[rest] for buf in (gas, gbs, ha_s, hb_s)]
    for n, part in enumerate(sent):
        remote(part, part, done.at[n], come.at[n], along(0, 1)).wait_send()


def write_out(a, b, c, d, a_out, b_out, c_out, d_out, sems):
    copies = [
        pltpu.make_async_copy(src, dst, sems.at[n])
        for n, (src, dst) in enumerate(((a, a_out), (b, b_out), (c, c_out), (d, d_out)))
    ]
    for copy in copies:
        copy.start()
    for copy in copies:
        copy.wait()


def body(queries, keys, values, cotangent, log_sum, chosen, normed_input):
    vm = pltpu.VMEM
    dma = pltpu.SemaphoreType.DMA
    scratch = [
        vm((4, 128, 128), BF16),
        vm((2, 8, 128, 128), BF16),
        vm((2, 8, 128, 128), BF16),
        vm((2, 8, 2, 128), F32),
        vm((8, 128, 256), BF16),
        vm((SEL, 2, 256), jnp.int32),
        vm((2, 128, 1024), BF16),
        vm((2, 128, 1024), BF16),
        vm((2, 64, 1024), BF16),
        vm((2048, 128), BF16),
        vm((2, 8, 4, 1024), F32),
        vm((2, 8, 128, 1024), F32),
        vm((2, 8, 128, 1024), F32),
        vm((2, 8, 128, 1024), BF16),
        vm((2, 8, 128, 1024), BF16),
        vm((2, 8, 8, 128), F32),
        vm((2, 8, 8, 128), F32),
        vm((2, 8, 128), F32),
    ]
    scratch += [vm((2, 8, 64, 128), BF16)] * 6
    scratch += [vm((8, 8, 16, 128), BF16)] * 4
    scratch += [vm((8, 16, 128), BF16)] * 4
    scratch += [dma((8,)), dma((2, 10)), dma((19,)), dma((19,))]
    shapes = (
        jax.ShapeDtypeStruct((TOK, COLS), BF16),
        jax.ShapeDtypeStruct((TOK, COLS), BF16),
        jax.ShapeDtypeStruct((TOK, COLS), BF16),
        jax.ShapeDtypeStruct((32, COLS), F32),
    )
    operands = (queries, keys, values, cotangent, log_sum, chosen.transpose(2, 0, 1), normed_input)
    inside = pl.pallas_call(
        kernel,
        out_shape=shapes,
        in_specs=[pl.BlockSpec(memory_space=pl.ANY)] * 7,
        out_specs=[pl.BlockSpec(memory_space=pltpu.VMEM)] * 4,
        scratch_shapes=scratch,
        compiler_params=pltpu.CompilerParams(
            collective_id=0, has_side_effects=True, vmem_limit_bytes=50 * 1024 * 1024
        ),
    )(*[pltpu.with_memory_space_constraint(operand, pltpu.HBM) for operand in operands])
    return pl.pallas_call(
        write_out,
        out_shape=shapes,
        in_specs=[pl.BlockSpec(memory_space=pltpu.VMEM)] * 4,
        out_specs=[pl.BlockSpec(memory_space=pl.ANY)] * 4,
        scratch_shapes=[dma((4,))],
        compiler_params=pltpu.CompilerParams(vmem_limit_bytes=4 * 1024 * 1024),
    )(*inside)


def solution(mesh):
    in_specs = (
        P("kv", "tp"),
        P("kv", "tp"),
        P("kv", "tp"),
        P("kv", "tp"),
        P("tp", "kv"),
        P("tp", None, None),
        P("kv", "tp"),
    )
    out_specs = (P("kv", "tp"), P("kv", "tp"), P("kv", "tp"), P("kv", "tp"))
    return jax.shard_map(body, mesh=mesh, in_specs=in_specs, out_specs=out_specs, check_vma=False)
```

```python
import jax
import jax.numpy as jnp
from jax import lax
from jax.experimental import pallas as pl
from jax.experimental.pallas import tpu as pltpu
from jax.sharding import PartitionSpec as P

HD = 64
BLK = 32
SEL = 12
MASKED = -1e30
RING = 8
TOK = 128
COLS = 128
ORDER = (0, 2, -2, 1, -1, 3, -3, 4)
POS = {off % RING: i for i, off in enumerate(ORDER)}
FAR = (4, 3, -3, 2, -2, 1, -1)
MESH = pl.DeviceIdType.MESH
F32 = jnp.float32
BF16 = jnp.bfloat16


def nt(a, b):
    return lax.dot_general(a, b, (((1,), (1,)), ((), ())), preferred_element_type=F32)


def nn(a, b):
    return lax.dot_general(a, b, (((1,), (0,)), ((), ())), preferred_element_type=F32)


def kernel(
    q_in, k_in, v_in, g_in, ls_in, ch_in, x_in,
    dq_out, dk_out, dv_out, gw_out,
    raw, qg, kv, ls, xg, chs, qmt, gmt, kt, xt, bias, wf, dpf, w16, ds16, da, dl, tot,
    dvs, dvr, dks, dkr, dqs, dqr, gas, gar, gbs, gbr, ha_s, ha_r, hb_s, hb_r,
    loc, gather, done, come,
):
    me = lax.axis_index("kv")
    tp = lax.axis_index("tp")
    z = me // RING
    y = me % RING

    def ring(base, off):
        return (base + off + RING) % RING

    def dev(axis, off):
        return z * RING + ring(y, off) if axis == 0 else ring(z, off) * RING + y

    def along(axis, off):
        return (dev(axis, off), tp)

    def remote(src, dst, send, recv, target):
        return pltpu.make_async_remote_copy(
            src_ref=src, dst_ref=dst, send_sem=send, recv_sem=recv, device_id=target, device_id_type=MESH
        )

    def slot(off):
        return POS[off % RING]

    barrier = pltpu.get_barrier_semaphore()
    greeted = [along(axis, off) for off in (1, -1, 2, -2) for axis in (0, 1)]
    greeted += [(me, ring(tp, off)) for off in range(1, RING)]
    for target in greeted:
        pl.semaphore_signal(barrier, inc=1, device_id=target, device_id_type=MESH)

    loads = [
        pltpu.make_async_copy(src, dst, loc.at[n])
        for n, (src, dst) in enumerate(
            (
                (q_in, raw.at[0]), (g_in, raw.at[1]), (k_in, raw.at[2]), (v_in, raw.at[3]),
                (ls_in, ls.at[0, 0]), (ls_in, ls.at[1, 0]), (x_in, xg.at[0]), (ch_in, chs),
            )
        )
    ]
    for c in loads:
        c.start()
    left = lax.broadcasted_iota(jnp.int32, (TOK, COLS), 1) < HD
    for n, buf in ((0, qg), (2, kv)):
        loads[n].wait()
        loads[n + 1].wait()
        a, b = raw[n].astype(F32), raw[n + 1].astype(F32)
        buf[0, 0] = jnp.where(left, a, pltpu.roll(b, HD, 1)).astype(BF16)
        buf[1, 0] = jnp.where(left, pltpu.roll(a, HD, 1), b).astype(BF16)
    for c in loads[4:]:
        c.wait()
    pl.semaphore_wait(barrier, len(greeted))

    def piece(axis, half):
        return (qg.at[axis], kv.at[1 - axis], ls.at[axis])[half]

    steps = [(half, axis, d) for half in (2, 0, 1) for axis in (0, 1) for d in (1, -1)]

    def group(off, half):
        near = (off + 4) % RING - 4
        return 3 * ((0 if near < 0 else 1) if abs(near) == 2 else {1: 2, 3: 3, 4: 4}[abs(near)]) + half

    def pass_on(axis, src, half, hop):
        buf = piece(axis, half)
        remote(
            buf.at[slot(src)],
            buf.at[slot(src - hop)],
            done.at[3 * axis + half],
            gather.at[axis, group(src - hop, half)],
            along(axis, hop),
        ).start()

    for half, axis, d in steps:
        pass_on(axis, 0, half, 2 * d)
    for half, axis, d in steps:
        pass_on(axis, 0, half, d)
    for off in range(1, RING):
        remote(xg.at[0], xg.at[RING - off], done.at[6], come.at[6], (me, ring(tp, off))).start()

    lane = lax.broadcasted_iota(jnp.int32, (1, TOK), 1) // BLK
    for h in range(2):
        own_id = jnp.concatenate([dev(h, off) * 4 + lane for off in ORDER], axis=1)
        spread = (lax.broadcasted_iota(jnp.int32, (256, 1024), 0) == own_id).astype(BF16)
        own_id = own_id.astype(F32)
        lists = nn(chs[:, h, :].astype(F32).astype(BF16), spread)
        for i, off in enumerate(ORDER):
            block = (lax.broadcasted_iota(jnp.int32, (4, 1024), 0) + dev(1 - h, off) * 4).astype(F32)
            hit = jnp.zeros((4, 1024), F32)
            for s in range(SEL):
                hit = jnp.where(block == lists[s : s + 1, :], 1.0, hit)
            hit = jnp.where(block < own_id, hit, 0.0)
            hit = jnp.where(block == own_id, 1.0, hit)
            bias[h, i] = jnp.where(hit > 0.5, 0.0, MASKED)

    for h in range(2):
        qmt[h, HD:COLS, :] = jnp.zeros((HD, 1024), BF16)
        gmt[h, 0:HD, :] = jnp.zeros((HD, 1024), BF16)
        da[h] = jnp.zeros((8, 8, TOK), F32)

    def stage(i):
        lanes = slice(i * TOK, (i + 1) * TOK)
        for h in range(2):
            turned = qg[h, i].astype(F32).T.astype(BF16)
            qmt[h, 0:HD, lanes] = turned[0:HD]
            gmt[h, HD:COLS, lanes] = turned[HD:COLS]
            kt[h, :, lanes] = kv[h, i].astype(F32).T[0:HD].astype(BF16)

    row_i = lax.broadcasted_iota(jnp.int32, (TOK, TOK), 0)
    col_i = lax.broadcasted_iota(jnp.int32, (TOK, TOK), 1)
    future = (row_i // BLK == col_i // BLK) & (row_i > col_i)
    diag_bias = jnp.where(future, MASKED, 0.0).astype(F32)

    def strip(i, lo, hi, diagonal=False):
        for h in range(2):
            tile = kv[h, i]
            for at in range(lo, hi, 2):
                end = min(at + 2, hi)
                s = nn(tile, qmt[h, :, at * TOK : end * TOK])
                dp = nn(tile, gmt[h, :, at * TOK : end * TOK])
                for j in range(at, end):
                    lanes = slice((j - at) * TOK, (j - at + 1) * TOK)
                    into = slice(j * TOK, (j + 1) * TOK)
                    rows = bias[h, i, :, into] - ls[h, j, h : h + 1, :]
                    rows = jnp.concatenate(
                        [jnp.broadcast_to(rows[b : b + 1], (BLK, TOK)) for b in range(4)], axis=0
                    )
                    x = s[:, lanes] * 0.125 + rows
                    if diagonal:
                        x = x + diag_bias
                    w = jnp.exp(x)
                    d = dp[:, lanes]
                    wf[h, i, :, into] = w
                    dpf[h, i, :, into] = d
                    w16[h, i, :, into] = w.astype(BF16)
                    da[h, j] += jnp.sum((w * d).reshape(16, 8, TOK), axis=0)

    def strips(first, last, lo, hi, unroll=1):
        def one(i, _):
            strip(i, lo, hi)
            return 0

        lax.fori_loop(first, last, one, 0, unroll=unroll)

    stage(0)
    strip(0, 0, 1, True)

    def arrive(axis, n, ref):
        remote(ref, ref, done.at[3 * axis], gather.at[axis, n], along(axis, 1)).wait_recv()

    rest = pl.ds(1, 7)
    for half, axis, d in steps:
        arrive(axis, group(-2 * d, half), piece(axis, half).at[slot(-2 * d)])
        if half % 2 == (d < 0):
            pass_on(axis, -2 * d, half, 2 * d)
        pass_on(axis, -2 * d, half, d)
    stage(1)
    stage(2)
    strips(1, 3, 0, 3)
    strip(0, 1, 3)
    for n, first in ((6, 3), (9, 5)):
        for axis in (0, 1):
            for half in (0, 1, 2):
                arrive(axis, n + half, piece(axis, half).at[pl.ds(first, 2)])
        stage(first)
        stage(first + 1)
        strips(first, first + 2, 0, first + 2)
        strips(0, first, first, first + 2)
    for axis in (0, 1):
        for half in (0, 1, 2):
            arrive(axis, 12 + half, piece(axis, half).at[7])
    stage(7)
    strip(7, 0, 8)
    strips(0, 7, 7, 8, unroll=7)

    for axis in (0, 1):
        for j, off in enumerate(ORDER):
            row = ring(y if axis == 0 else z, off)
            dl[axis, 0, pl.ds(row, 1), :] = jnp.sum(da[axis, j], axis=0, keepdims=True)
    for off in FAR:
        for axis in (0, 1):
            remote(
                dl.at[axis, 0], dl.at[axis, slot(-off)], done.at[7 + axis], come.at[7 + axis], along(axis, off)
            ).start()

    def scatter(buf, into, h, axis, n):
        for off in FAR:
            remote(
                buf.at[h, slot(off)], into.at[h, slot(-off)], done.at[n + h], come.at[n + h], along(axis, off)
            ).start()

    def value_grad(i, _):
        for h in range(2):
            dvs[h, i] = nt(gmt[h, HD:COLS, :], w16[h, i]).astype(BF16)
        return 0

    lax.fori_loop(0, RING, value_grad, 0, unroll=4)
    for h in range(2):
        scatter(dvs, dvr, h, 1 - h, 9)

    part = xg.at[rest]
    remote(part, part, done.at[6], come.at[6], (me, ring(tp, 1))).wait_recv()
    for o in range(RING):
        xt[pl.ds(pl.multiple_of(ring(tp, o) * 256, 256), 256), :] = xg[o].astype(F32).T.astype(BF16)

    for axis in (0, 1):
        part = dl.at[axis, rest]
        remote(part, part, done.at[7 + axis], come.at[7 + axis], along(axis, 1)).wait_recv()
        acc = dl[axis, 0]
        for n in range(1, RING):
            acc = acc + dl[axis, n]
        tot[axis] = acc

    for lo, hi in ((7, 8), (5, 7), (1, 3), (3, 5), (0, 1)):
        into = slice(lo * TOK, hi * TOK)
        for h in range(2):
            delta = jnp.concatenate(
                [tot[h, pl.ds(ring(y if h == 0 else z, ORDER[j]), 1), :] for j in range(lo, hi)], axis=1
            )
            acc = jnp.zeros((HD, (hi - lo) * TOK), F32)
            for i in range(0, RING, 2):
                pair = []
                for n in (i, i + 1):
                    low = (wf[h, n, :, into] * (dpf[h, n, :, into] - delta)).astype(BF16)
                    ds16[h, n, :, into] = low
                    pair.append(low)
                acc = acc + nn(kt[h, :, i * TOK : (i + 2) * TOK], jnp.concatenate(pair, axis=0))
            for j in range(lo, hi):
                dqs[h, j] = acc[:, (j - lo) * TOK : (j - lo + 1) * TOK].astype(BF16)
        for j in range(max(lo, 1), hi):
            for h in range(2):
                remote(
                    dqs.at[h, j], dqr.at[h, slot(-ORDER[j])], done.at[11 + h], come.at[11 + h], along(h, ORDER[j])
                ).start()

    def key_grad(i, _):
        for h in range(2):
            dks[h, i] = nt(qmt[h, 0:HD, :], ds16[h, i]).astype(BF16)
        return 0

    lax.fori_loop(0, RING, key_grad, 0, unroll=4)
    for h in range(2):
        scatter(dks, dkr, h, 1 - h, 13)

    def both_heads(own, arrived, n):
        sums = []
        for h in range(2):
            part = arrived.at[h, rest]
            remote(part, part, done.at[n + h], come.at[n + h], along(0, 1)).wait_recv()
            acc = own[h, 0].astype(F32)
            for i in range(1, RING):
                acc = acc + arrived[h, i].astype(F32)
            sums.append(acc)
        return jnp.concatenate(sums, axis=0).T

    dq = (both_heads(dqs, dqr, 11) * 0.125).astype(BF16)
    dq_out[...] = dq

    def weight_part(zz, _):
        part = nn(xt[pl.ds(pl.multiple_of(zz * 256, 256), 256), :], dq)
        part = part.astype(BF16).reshape(RING, 2, 16, COLS)
        gas[zz] = part[:, 0]
        gbs[:, zz] = part[:, 1]
        return 0

    lax.fori_loop(0, RING, weight_part, 0, unroll=4)
    for off in FAR:
        remote(gas.at[ring(z, off)], gar.at[slot(-off)], done.at[15], come.at[15], along(1, off)).start()
        remote(gbs.at[ring(y, off)], gbr.at[slot(-off)], done.at[16], come.at[16], along(0, off)).start()

    dv_out[...] = both_heads(dvs, dvr, 9).astype(BF16)
    dk_out[...] = (both_heads(dks, dkr, 13) * 0.125).astype(BF16)

    def summed(own, arrived, n):
        part = arrived.at[rest]
        remote(part, part, done.at[n], come.at[n], along(0, 1)).wait_recv()
        acc = own.astype(F32)
        for i in range(1, RING):
            acc = acc + arrived[i].astype(F32)
        return acc

    ha_s[...] = summed(gas[z], gar, 15).astype(BF16)
    for off in FAR:
        remote(ha_s.at[ring(y, off)], ha_r.at[slot(-off)], done.at[17], come.at[17], along(0, off)).start()
    hb_s[...] = summed(gbs[y], gbr, 16).astype(BF16)
    for off in FAR:
        remote(hb_s.at[ring(z, off)], hb_r.at[slot(-off)], done.at[18], come.at[18], along(1, off)).start()
    gw_out[0:16, :] = summed(ha_s[y], ha_r, 17)
    gw_out[16:32, :] = summed(hb_s[z], hb_r, 18)

    sent = [qg.at[0, rest], kv.at[1, rest], ls.at[0, rest], qg.at[1, rest], kv.at[0, rest], ls.at[1, rest]]
    sent += [xg.at[rest], dl.at[0, rest], dl.at[1, rest]]
    sent += [buf.at[h, rest] for buf in (dvs, dqs, dks) for h in range(2)]
    sent += [buf.at[rest] for buf in (gas, gbs, ha_s, hb_s)]
    for n, part in enumerate(sent):
        remote(part, part, done.at[n], come.at[n], along(0, 1)).wait_send()


def write_out(a, b, c, d, a_out, b_out, c_out, d_out, sems):
    copies = [
        pltpu.make_async_copy(src, dst, sems.at[n])
        for n, (src, dst) in enumerate(((a, a_out), (b, b_out), (c, c_out), (d, d_out)))
    ]
    for copy in copies:
        copy.start()
    for copy in copies:
        copy.wait()


def body(queries, keys, values, cotangent, log_sum, chosen, normed_input):
    vm = pltpu.VMEM
    dma = pltpu.SemaphoreType.DMA
    scratch = [
        vm((4, 128, 128), BF16),
        vm((2, 8, 128, 128), BF16),
        vm((2, 8, 128, 128), BF16),
        vm((2, 8, 2, 128), F32),
        vm((8, 128, 256), BF16),
        vm((SEL, 2, 256), jnp.int32),
        vm((2, 128, 1024), BF16),
        vm((2, 128, 1024), BF16),
        vm((2, 64, 1024), BF16),
        vm((2048, 128), BF16),
        vm((2, 8, 4, 1024), F32),
        vm((2, 8, 128, 1024), F32),
        vm((2, 8, 128, 1024), F32),
        vm((2, 8, 128, 1024), BF16),
        vm((2, 8, 128, 1024), BF16),
        vm((2, 8, 8, 128), F32),
        vm((2, 8, 8, 128), F32),
        vm((2, 8, 128), F32),
    ]
    scratch += [vm((2, 8, 64, 128), BF16)] * 6
    scratch += [vm((8, 8, 16, 128), BF16)] * 4
    scratch += [vm((8, 16, 128), BF16)] * 4
    scratch += [dma((8,)), dma((2, 15)), dma((19,)), dma((19,))]
    shapes = (
        jax.ShapeDtypeStruct((TOK, COLS), BF16),
        jax.ShapeDtypeStruct((TOK, COLS), BF16),
        jax.ShapeDtypeStruct((TOK, COLS), BF16),
        jax.ShapeDtypeStruct((32, COLS), F32),
    )
    operands = (queries, keys, values, cotangent, log_sum, chosen.transpose(2, 0, 1), normed_input)
    inside = pl.pallas_call(
        kernel,
        out_shape=shapes,
        in_specs=[pl.BlockSpec(memory_space=pl.ANY)] * 7,
        out_specs=[pl.BlockSpec(memory_space=pltpu.VMEM)] * 4,
        scratch_shapes=scratch,
        compiler_params=pltpu.CompilerParams(
            collective_id=0, has_side_effects=True, vmem_limit_bytes=50 * 1024 * 1024
        ),
    )(*[pltpu.with_memory_space_constraint(operand, pltpu.HBM) for operand in operands])
    return pl.pallas_call(
        write_out,
        out_shape=shapes,
        in_specs=[pl.BlockSpec(memory_space=pltpu.VMEM)] * 4,
        out_specs=[pl.BlockSpec(memory_space=pl.ANY)] * 4,
        scratch_shapes=[dma((4,))],
        compiler_params=pltpu.CompilerParams(vmem_limit_bytes=4 * 1024 * 1024),
    )(*inside)


def solution(mesh):
    in_specs = (
        P("kv", "tp"),
        P("kv", "tp"),
        P("kv", "tp"),
        P("kv", "tp"),
        P("tp", "kv"),
        P("tp", None, None),
        P("kv", "tp"),
    )
    out_specs = (P("kv", "tp"), P("kv", "tp"), P("kv", "tp"), P("kv", "tp"))
    return jax.shard_map(body, mesh=mesh, in_specs=in_specs, out_specs=out_specs, check_vma=False)
```

```python
import jax
import jax.numpy as jnp
from jax import lax
from jax.experimental import pallas as pl
from jax.experimental.pallas import tpu as pltpu
from jax.sharding import PartitionSpec as P

HD = 64
BLK = 32
SEL = 12
MASKED = -1e30
RING = 8
TOK = 128
COLS = 128
ORDER = (0, 2, -2, 1, -1, 3, -3, 4)
POS = {off % RING: i for i, off in enumerate(ORDER)}
FAR = (4, 3, -3, 2, -2, 1, -1)
MESH = pl.DeviceIdType.MESH
F32 = jnp.float32
BF16 = jnp.bfloat16


def nt(a, b):
    return lax.dot_general(a, b, (((1,), (1,)), ((), ())), preferred_element_type=F32)


def nn(a, b):
    return lax.dot_general(a, b, (((1,), (0,)), ((), ())), preferred_element_type=F32)


def kernel(
    q_in, k_in, v_in, g_in, ls_in, ch_in, x_in,
    dq_out, dk_out, dv_out, gw_out,
    raw, qg, kv, ls, xg, chs, qmt, gmt, kt, xt, bias, wf, dpf, w16, ds16, da, dl, tot,
    dvs, dvr, dks, dkr, dqs, dqr, gas, gar, gbs, gbr, ha_s, ha_r, hb_s, hb_r,
    loc, gather, done, come,
):
    me = lax.axis_index("kv")
    tp = lax.axis_index("tp")
    z = me // RING
    y = me % RING

    def ring(base, off):
        return (base + off + RING) % RING

    def dev(axis, off):
        return z * RING + ring(y, off) if axis == 0 else ring(z, off) * RING + y

    def along(axis, off):
        return (dev(axis, off), tp)

    def remote(src, dst, send, recv, target):
        return pltpu.make_async_remote_copy(
            src_ref=src, dst_ref=dst, send_sem=send, recv_sem=recv, device_id=target, device_id_type=MESH
        )

    def slot(off):
        return POS[off % RING]

    barrier = pltpu.get_barrier_semaphore()
    greeted = [along(axis, off) for off in (1, -1, 2, -2) for axis in (0, 1)]
    greeted += [(me, ring(tp, off)) for off in range(1, RING)]
    for target in greeted:
        pl.semaphore_signal(barrier, inc=1, device_id=target, device_id_type=MESH)

    loads = [
        pltpu.make_async_copy(src, dst, loc.at[n])
        for n, (src, dst) in enumerate(
            (
                (q_in, raw.at[0]), (g_in, raw.at[1]), (k_in, raw.at[2]), (v_in, raw.at[3]),
                (ls_in, ls.at[0, 0]), (ls_in, ls.at[1, 0]), (x_in, xg.at[0]), (ch_in, chs),
            )
        )
    ]
    for c in loads:
        c.start()
    left = lax.broadcasted_iota(jnp.int32, (TOK, COLS), 1) < HD
    for n, buf in ((0, qg), (2, kv)):
        loads[n].wait()
        loads[n + 1].wait()
        a, b = raw[n].astype(F32), raw[n + 1].astype(F32)
        buf[0, 0] = jnp.where(left, a, pltpu.roll(b, HD, 1)).astype(BF16)
        buf[1, 0] = jnp.where(left, pltpu.roll(a, HD, 1), b).astype(BF16)
    loads[4].wait()
    loads[5].wait()
    pl.semaphore_wait(barrier, len(greeted))

    def piece(axis, half):
        return (qg.at[axis], kv.at[1 - axis], ls.at[axis])[half]

    steps = [(half, axis, d) for half in (2, 0, 1) for axis in (0, 1) for d in (1, -1)]

    def group(off, half):
        near = (off + 4) % RING - 4
        return 3 * ((0 if near < 0 else 1) if abs(near) == 2 else {1: 2, 3: 3, 4: 4}[abs(near)]) + half

    def pass_on(axis, src, half, hop):
        buf = piece(axis, half)
        remote(
            buf.at[slot(src)],
            buf.at[slot(src - hop)],
            done.at[3 * axis + half],
            gather.at[axis, group(src - hop, half)],
            along(axis, hop),
        ).start()

    for half, axis, d in steps:
        pass_on(axis, 0, half, 2 * d)
    for half, axis, d in steps:
        pass_on(axis, 0, half, d)
    loads[6].wait()
    loads[7].wait()
    for off in range(1, RING):
        remote(xg.at[0], xg.at[RING - off], done.at[6], come.at[6], (me, ring(tp, off))).start()

    lane = lax.broadcasted_iota(jnp.int32, (1, TOK), 1) // BLK
    for h in range(2):
        own_id = jnp.concatenate([dev(h, off) * 4 + lane for off in ORDER], axis=1)
        spread = (lax.broadcasted_iota(jnp.int32, (256, 1024), 0) == own_id).astype(BF16)
        own_id = own_id.astype(F32)
        lists = nn(chs[:, h, :].astype(F32).astype(BF16), spread)
        for i, off in enumerate(ORDER):
            block = (lax.broadcasted_iota(jnp.int32, (4, 1024), 0) + dev(1 - h, off) * 4).astype(F32)
            hit = jnp.zeros((4, 1024), F32)
            for s in range(SEL):
                hit = jnp.where(block == lists[s : s + 1, :], 1.0, hit)
            hit = jnp.where(block < own_id, hit, 0.0)
            hit = jnp.where(block == own_id, 1.0, hit)
            bias[h, i] = jnp.where(hit > 0.5, 0.0, MASKED)

    for h in range(2):
        qmt[h, HD:COLS, :] = jnp.zeros((HD, 1024), BF16)
        gmt[h, 0:HD, :] = jnp.zeros((HD, 1024), BF16)
        da[h] = jnp.zeros((8, 8, TOK), F32)

    def stage(i):
        lanes = slice(i * TOK, (i + 1) * TOK)
        for h in range(2):
            turned = qg[h, i].astype(F32).T.astype(BF16)
            qmt[h, 0:HD, lanes] = turned[0:HD]
            gmt[h, HD:COLS, lanes] = turned[HD:COLS]
            kt[h, :, lanes] = kv[h, i].astype(F32).T[0:HD].astype(BF16)

    row_i = lax.broadcasted_iota(jnp.int32, (TOK, TOK), 0)
    col_i = lax.broadcasted_iota(jnp.int32, (TOK, TOK), 1)
    future = (row_i // BLK == col_i // BLK) & (row_i > col_i)
    diag_bias = jnp.where(future, MASKED, 0.0).astype(F32)

    def strip(i, lo, hi, diagonal=False):
        for h in range(2):
            tile = kv[h, i]
            for at in range(lo, hi, 2):
                end = min(at + 2, hi)
                s = nn(tile, qmt[h, :, at * TOK : end * TOK])
                dp = nn(tile, gmt[h, :, at * TOK : end * TOK])
                for j in range(at, end):
                    lanes = slice((j - at) * TOK, (j - at + 1) * TOK)
                    into = slice(j * TOK, (j + 1) * TOK)
                    rows = bias[h, i, :, into] - ls[h, j, h : h + 1, :]
                    rows = jnp.concatenate(
                        [jnp.broadcast_to(rows[b : b + 1], (BLK, TOK)) for b in range(4)], axis=0
                    )
                    x = s[:, lanes] * 0.125 + rows
                    if diagonal:
                        x = x + diag_bias
                    w = jnp.exp(x)
                    d = dp[:, lanes]
                    wf[h, i, :, into] = w
                    dpf[h, i, :, into] = d
                    w16[h, i, :, into] = w.astype(BF16)
                    da[h, j] += jnp.sum((w * d).reshape(16, 8, TOK), axis=0)

    def strips(first, last, lo, hi, unroll=2):
        def one(i, _):
            strip(i, lo, hi)
            return 0

        lax.fori_loop(first, last, one, 0, unroll=unroll)

    stage(0)
    strip(0, 0, 1, True)

    def arrive(axis, n, ref):
        remote(ref, ref, done.at[3 * axis], gather.at[axis, n], along(axis, 1)).wait_recv()

    rest = pl.ds(1, 7)
    for half, axis, d in steps:
        arrive(axis, group(-2 * d, half), piece(axis, half).at[slot(-2 * d)])
        if half % 2 == (d < 0):
            pass_on(axis, -2 * d, half, 2 * d)
        pass_on(axis, -2 * d, half, d)
    stage(1)
    stage(2)
    strips(1, 3, 0, 3)
    strip(0, 1, 3)
    for n, first in ((6, 3), (9, 5)):
        for axis in (0, 1):
            for half in (0, 1, 2):
                arrive(axis, n + half, piece(axis, half).at[pl.ds(first, 2)])
        stage(first)
        stage(first + 1)
        strips(first, first + 2, 0, first + 2)
        strips(0, first, first, first + 2)
    for axis in (0, 1):
        for half in (0, 1, 2):
            arrive(axis, 12 + half, piece(axis, half).at[7])
    stage(7)
    strip(7, 0, 8)
    strips(0, 7, 7, 8, unroll=7)

    for axis in (0, 1):
        for j, off in enumerate(ORDER):
            row = ring(y if axis == 0 else z, off)
            dl[axis, 0, pl.ds(row, 1), :] = jnp.sum(da[axis, j], axis=0, keepdims=True)
    for off in FAR:
        for axis in (0, 1):
            remote(
                dl.at[axis, 0], dl.at[axis, slot(-off)], done.at[7 + axis], come.at[7 + axis], along(axis, off)
            ).start()

    def scatter(buf, into, h, axis, n):
        for off in FAR:
            remote(
                buf.at[h, slot(off)], into.at[h, slot(-off)], done.at[n + h], come.at[n + h], along(axis, off)
            ).start()

    def value_grad(i, _):
        for h in range(2):
            dvs[h, i] = nt(gmt[h, HD:COLS, :], w16[h, i]).astype(BF16)
        return 0

    lax.fori_loop(0, RING, value_grad, 0, unroll=4)
    for h in range(2):
        scatter(dvs, dvr, h, 1 - h, 9)

    part = xg.at[rest]
    remote(part, part, done.at[6], come.at[6], (me, ring(tp, 1))).wait_recv()
    for o in range(RING):
        xt[pl.ds(pl.multiple_of(ring(tp, o) * 256, 256), 256), :] = xg[o].astype(F32).T.astype(BF16)

    for axis in (0, 1):
        part = dl.at[axis, rest]
        remote(part, part, done.at[7 + axis], come.at[7 + axis], along(axis, 1)).wait_recv()
        acc = dl[axis, 0]
        for n in range(1, RING):
            acc = acc + dl[axis, n]
        tot[axis] = acc

    for lo, hi in ((7, 8), (5, 7), (1, 3), (3, 5), (0, 1)):
        into = slice(lo * TOK, hi * TOK)
        for h in range(2):
            delta = jnp.concatenate(
                [tot[h, pl.ds(ring(y if h == 0 else z, ORDER[j]), 1), :] for j in range(lo, hi)], axis=1
            )
            acc = jnp.zeros((HD, (hi - lo) * TOK), F32)
            for i in range(0, RING, 2):
                pair = []
                for n in (i, i + 1):
                    low = (wf[h, n, :, into] * (dpf[h, n, :, into] - delta)).astype(BF16)
                    ds16[h, n, :, into] = low
                    pair.append(low)
                acc = acc + nn(kt[h, :, i * TOK : (i + 2) * TOK], jnp.concatenate(pair, axis=0))
            for j in range(lo, hi):
                dqs[h, j] = acc[:, (j - lo) * TOK : (j - lo + 1) * TOK].astype(BF16)
        for j in range(max(lo, 1), hi):
            for h in range(2):
                remote(
                    dqs.at[h, j], dqr.at[h, slot(-ORDER[j])], done.at[11 + h], come.at[11 + h], along(h, ORDER[j])
                ).start()

    def key_grad(i, _):
        for h in range(2):
            dks[h, i] = nt(qmt[h, 0:HD, :], ds16[h, i]).astype(BF16)
        return 0

    lax.fori_loop(0, RING, key_grad, 0, unroll=4)
    for h in range(2):
        scatter(dks, dkr, h, 1 - h, 13)

    def both_heads(own, arrived, n):
        sums = []
        for h in range(2):
            part = arrived.at[h, rest]
            remote(part, part, done.at[n + h], come.at[n + h], along(0, 1)).wait_recv()
            acc = own[h, 0].astype(F32)
            for i in range(1, RING):
                acc = acc + arrived[h, i].astype(F32)
            sums.append(acc)
        return jnp.concatenate(sums, axis=0).T

    dq = (both_heads(dqs, dqr, 11) * 0.125).astype(BF16)
    dq_out[...] = dq

    def weight_part(zz, _):
        part = nn(xt[pl.ds(pl.multiple_of(zz * 256, 256), 256), :], dq)
        part = part.astype(BF16).reshape(RING, 2, 16, COLS)
        gas[zz] = part[:, 0]
        gbs[:, zz] = part[:, 1]
        return 0

    lax.fori_loop(0, RING, weight_part, 0, unroll=4)
    for off in FAR:
        remote(gas.at[ring(z, off)], gar.at[slot(-off)], done.at[15], come.at[15], along(1, off)).start()
        remote(gbs.at[ring(y, off)], gbr.at[slot(-off)], done.at[16], come.at[16], along(0, off)).start()

    dv_out[...] = both_heads(dvs, dvr, 9).astype(BF16)

    def summed(own, arrived, n):
        part = arrived.at[rest]
        remote(part, part, done.at[n], come.at[n], along(0, 1)).wait_recv()
        acc = own.astype(F32)
        for i in range(1, RING):
            acc = acc + arrived[i].astype(F32)
        return acc

    ha_s[...] = summed(gas[z], gar, 15).astype(BF16)
    for off in FAR:
        remote(ha_s.at[ring(y, off)], ha_r.at[slot(-off)], done.at[17], come.at[17], along(0, off)).start()
    hb_s[...] = summed(gbs[y], gbr, 16).astype(BF16)
    for off in FAR:
        remote(hb_s.at[ring(z, off)], hb_r.at[slot(-off)], done.at[18], come.at[18], along(1, off)).start()
    dk_out[...] = (both_heads(dks, dkr, 13) * 0.125).astype(BF16)
    gw_out[0:16, :] = summed(ha_s[y], ha_r, 17)
    gw_out[16:32, :] = summed(hb_s[z], hb_r, 18)

    sent = [qg.at[0, rest], kv.at[1, rest], ls.at[0, rest], qg.at[1, rest], kv.at[0, rest], ls.at[1, rest]]
    sent += [xg.at[rest], dl.at[0, rest], dl.at[1, rest]]
    sent += [buf.at[h, rest] for buf in (dvs, dqs, dks) for h in range(2)]
    sent += [buf.at[rest] for buf in (gas, gbs, ha_s, hb_s)]
    for n, part in enumerate(sent):
        remote(part, part, done.at[n], come.at[n], along(0, 1)).wait_send()


def write_out(a, b, c, d, a_out, b_out, c_out, d_out, sems):
    copies = [
        pltpu.make_async_copy(src, dst, sems.at[n])
        for n, (src, dst) in enumerate(((a, a_out), (b, b_out), (c, c_out), (d, d_out)))
    ]
    for copy in copies:
        copy.start()
    for copy in copies:
        copy.wait()


def body(queries, keys, values, cotangent, log_sum, chosen, normed_input):
    vm = pltpu.VMEM
    dma = pltpu.SemaphoreType.DMA
    scratch = [
        vm((4, 128, 128), BF16),
        vm((2, 8, 128, 128), BF16),
        vm((2, 8, 128, 128), BF16),
        vm((2, 8, 2, 128), F32),
        vm((8, 128, 256), BF16),
        vm((SEL, 2, 256), jnp.int32),
        vm((2, 128, 1024), BF16),
        vm((2, 128, 1024), BF16),
        vm((2, 64, 1024), BF16),
        vm((2048, 128), BF16),
        vm((2, 8, 4, 1024), F32),
        vm((2, 8, 128, 1024), F32),
        vm((2, 8, 128, 1024), F32),
        vm((2, 8, 128, 1024), BF16),
        vm((2, 8, 128, 1024), BF16),
        vm((2, 8, 8, 128), F32),
        vm((2, 8, 8, 128), F32),
        vm((2, 8, 128), F32),
    ]
    scratch += [vm((2, 8, 64, 128), BF16)] * 6
    scratch += [vm((8, 8, 16, 128), BF16)] * 4
    scratch += [vm((8, 16, 128), BF16)] * 4
    scratch += [dma((8,)), dma((2, 15)), dma((19,)), dma((19,))]
    shapes = (
        jax.ShapeDtypeStruct((TOK, COLS), BF16),
        jax.ShapeDtypeStruct((TOK, COLS), BF16),
        jax.ShapeDtypeStruct((TOK, COLS), BF16),
        jax.ShapeDtypeStruct((32, COLS), F32),
    )
    operands = (queries, keys, values, cotangent, log_sum, chosen.transpose(2, 0, 1), normed_input)
    inside = pl.pallas_call(
        kernel,
        out_shape=shapes,
        in_specs=[pl.BlockSpec(memory_space=pl.ANY)] * 7,
        out_specs=[pl.BlockSpec(memory_space=pltpu.VMEM)] * 4,
        scratch_shapes=scratch,
        compiler_params=pltpu.CompilerParams(
            collective_id=0, has_side_effects=True, vmem_limit_bytes=50 * 1024 * 1024
        ),
    )(*[pltpu.with_memory_space_constraint(operand, pltpu.HBM) for operand in operands])
    return pl.pallas_call(
        write_out,
        out_shape=shapes,
        in_specs=[pl.BlockSpec(memory_space=pltpu.VMEM)] * 4,
        out_specs=[pl.BlockSpec(memory_space=pl.ANY)] * 4,
        scratch_shapes=[dma((4,))],
        compiler_params=pltpu.CompilerParams(vmem_limit_bytes=4 * 1024 * 1024),
    )(*inside)


def solution(mesh):
    in_specs = (
        P("kv", "tp"),
        P("kv", "tp"),
        P("kv", "tp"),
        P("kv", "tp"),
        P("tp", "kv"),
        P("tp", None, None),
        P("kv", "tp"),
    )
    out_specs = (P("kv", "tp"), P("kv", "tp"), P("kv", "tp"), P("kv", "tp"))
    return jax.shard_map(body, mesh=mesh, in_specs=in_specs, out_specs=out_specs, check_vma=False)
```
